32 devices in a mesh: sp: 8 (over z, x), tp: 4 (over y, core).
Axes of the slice: x: 2, y: 2, z: 4, core: 2. Of those that a mesh axis runs over, the one named last changes fastest.
Arguments:
- residual: bfloat16 [1024, 2048], P(('sp', 'tp')), may hold values from -6 to 6
- query_first: bfloat16 [1024, 1024], P('sp', 'tp'), may hold values from -200 to 200
- key_first: bfloat16 [1024, 1024], P('sp', 'tp'), may hold values from -200 to 200
- query_second: bfloat16 [1024, 1024], P('sp', 'tp'), may hold values from -200 to 200
- key_second: bfloat16 [1024, 1024], P('sp', 'tp'), may hold values from -200 to 200
- values: bfloat16 [1024, 2048], P('sp', 'tp'), may hold values from -6 to 6
- lambda_weight: float32 [16], P('tp'), may hold values from 0.3 to 0.8
- head_gain: float32 [128], replicated, may hold values from 0.1 to 1.9
- out_weight: bfloat16 [2048, 2048], P('sp', 'tp'), may hold values from -0.125 to 0.125
- norm_gain: float32 [2048], replicated, may hold values from 0.1 to 1.9
- gate_weight: bfloat16 [2048, 5632], P(None, 'tp'), may hold values from -0.125 to 0.125
- up_weight: bfloat16 [2048, 5632], P(None, 'tp'), may hold values from -0.125 to 0.125
- down_weight: bfloat16 [2048, 5632], P('sp', 'tp'), may hold values from -0.078125 to 0.078125
Outputs:
- layer_out: bfloat16 [1024, 2048], P(('sp', 'tp'))
The draws below stay inside these ranges and needn't reach their ends.
All inputs are finite; a program needn't handle non-finite values.
Results may differ from the reference program's by a relative error of at most 0.017.
Values may be sent and summed in bfloat16 or wider, within the bound.
No kernel may reach another device: no remote copies, remote signals or barrier semaphores. Data moves between devices by JAX's collectives and lax.ppermute only.
A program may use at most 128 MiB of HBM per device.

```python
import jax
import jax.numpy as jnp
from jax import lax

D = 2048
HEADS = 16
HD = 64
VD = 128
FF = 5632
TOKENS = 1024
N_TP = 4


def plant_pair(key, which):
    spread = 1.32
    key_rows = jax.random.normal(jax.random.fold_in(key, 101 + which), (TOKENS, HEADS * HD), jnp.float32) * spread
    key_rows = jnp.clip(key_rows, -6.0 * spread, 6.0 * spread)
    queries = jax.random.normal(jax.random.fold_in(key, 201 + which), (TOKENS, HEADS * HD), jnp.float32) * spread
    queries = jnp.clip(queries, -6.0 * spread, 6.0 * spread)
    return (queries, key_rows)


def draw_query_first(key, part):
    return plant_pair(key, 0)[0].astype(jnp.bfloat16)


def draw_key_first(key, part):
    return plant_pair(key, 0)[1].astype(jnp.bfloat16)


def draw_query_second(key, part):
    return plant_pair(key, 1)[0].astype(jnp.bfloat16)


def draw_key_second(key, part):
    return plant_pair(key, 1)[1].astype(jnp.bfloat16)


def shard_levels(rng, shape, cuts, low, high):
    def one(axis_at, blocks):
        steps = jax.random.uniform(jax.random.fold_in(jax.random.fold_in(rng, 6), axis_at), (blocks,), jnp.float32, low / len(cuts), high / len(cuts))
        return jnp.repeat(jnp.exp(steps), shape[axis_at] // blocks).reshape((-1,) + (1,) * (len(shape) - axis_at - 1))

    level = one(*cuts[0])
    for cut in cuts[1:]:
        level = level * one(*cut)
    return level


def normal_values(stream_key, extent, deviation, reach, cuts=(), held_as=jnp.bfloat16):
    loudness = shard_levels(stream_key, extent, cuts, -0.22, 0.18) if cuts else 1.0
    values = jax.random.normal(stream_key, extent, jnp.float32) * deviation * loudness
    return jnp.minimum(jnp.maximum(values, -reach), reach).astype(held_as)


def setup_inputs(seed: int = 0) -> dict:
    arg_keys = jax.random.split(jax.random.key(seed), 14)
    residual = normal_values(arg_keys[0], (TOKENS, D), 1.0, 6.0, ((0, 32),))
    query_first = draw_query_first(jax.random.fold_in(arg_keys[13], 71), 0)
    key_first = draw_key_first(jax.random.fold_in(arg_keys[13], 71), 0)
    query_second = draw_query_second(jax.random.fold_in(arg_keys[13], 71), 0)
    key_second = draw_key_second(jax.random.fold_in(arg_keys[13], 71), 0)
    values = normal_values(arg_keys[5], (TOKENS, HEADS * VD), 1.0, 6.0, ((0, 8), (1, 4)))
    lambda_weight = jnp.clip(0.3 + 0.5 * jax.random.uniform(arg_keys[6], (HEADS,), jnp.float32) ** shard_levels(arg_keys[6], (HEADS,), ((0, 4),), -0.2, 0.2), 0.3, 0.8)
    head_gain = jnp.clip(1.0 + 0.18 * jax.random.normal(arg_keys[7], (VD,), jnp.float32), 0.1, 1.9)
    out_weight = normal_values(arg_keys[8], (D, HEADS * VD), (HEADS * VD) ** -0.5, 0.125, ((0, 8), (1, 4)))
    norm_gain = jnp.clip(1.0 + 0.18 * jax.random.normal(arg_keys[9], (D,), jnp.float32), 0.1, 1.9)
    gate_weight = normal_values(arg_keys[10], (D, FF), D ** -0.5, 0.125, ((1, 4),))
    up_weight = normal_values(arg_keys[11], (D, FF), D ** -0.5, 0.125, ((1, 4),))
    down_weight = normal_values(arg_keys[12], (D, FF), FF ** -0.5, 0.078125, ((0, 8), (1, 4)))
    return {"residual": residual, "query_first": query_first, "key_first": key_first, "query_second": query_second, "key_second": key_second, "values": values, "lambda_weight": lambda_weight, "head_gain": head_gain, "out_weight": out_weight, "norm_gain": norm_gain, "gate_weight": gate_weight, "up_weight": up_weight, "down_weight": down_weight}


epsilon = 1e-06

def one_map(queries, key_rows, value_rows):
    scores = jnp.dot(queries, key_rows.T, preferred_element_type=jnp.float32) * queries.shape[-1] ** (-0.5)
    shifted = jnp.exp(scores - lax.optimization_barrier(jnp.max(scores, axis=-1, keepdims=True)))
    totals = lax.optimization_barrier(jnp.sum(shifted, axis=-1, keepdims=True))
    product = jnp.dot(shifted.astype(jnp.bfloat16), value_rows, preferred_element_type=jnp.float32)
    return product / totals

def attend_head(inputs, head_gain):
    query_one, key_one, query_two, key_two, value_rows, weight = inputs
    first_map = one_map(query_one, key_one, value_rows)
    second_map = one_map(query_two, key_two, value_rows)
    difference = first_map - weight * second_map
    scaled = difference * lax.rsqrt(lax.optimization_barrier(jnp.mean(difference * difference, axis=-1, keepdims=True)) + epsilon)
    return (scaled * head_gain).astype(jnp.bfloat16)

def reference(residual, query_first, key_first, query_second, key_second, values, lambda_weight, head_gain, out_weight, norm_gain, gate_weight, up_weight, down_weight):
    length = query_first.shape[0]

    def split_heads(array, entries):
        return array.reshape(length, HEADS, entries).transpose(1, 0, 2)
    stacked = (split_heads(query_first, HD), split_heads(key_first, HD), split_heads(query_second, HD), split_heads(key_second, HD), split_heads(values, VD), lambda_weight)
    heads_out = lax.map(lambda inputs: attend_head(inputs, head_gain), stacked)
    attended = heads_out.transpose(1, 0, 2).reshape(length, HEADS * VD)
    group_width = HEADS * VD // N_TP
    projected = jnp.zeros((length, D), jnp.float32)
    for member in range(N_TP):
        columns = slice(member * group_width, (member + 1) * group_width)
        partial_value = lax.dot_general(attended[:, columns], out_weight[:, columns], (((1,), (1,)), ((), ())), preferred_element_type=jnp.float32)
        projected = projected + lax.optimization_barrier(partial_value.astype(jnp.bfloat16)).astype(jnp.float32)
    after_attention = (residual.astype(jnp.float32) + projected).astype(jnp.bfloat16)
    stream = after_attention.astype(jnp.float32)
    normed = (stream * lax.rsqrt(lax.optimization_barrier(jnp.mean(stream * stream, axis=-1, keepdims=True)) + epsilon) * norm_gain).astype(jnp.bfloat16)
    hidden_width = FF // N_TP
    feed_sum = jnp.zeros((length, D), jnp.float32)
    for member in range(N_TP):
        columns = slice(member * hidden_width, (member + 1) * hidden_width)
        gate_part = jnp.dot(normed, gate_weight[:, columns], preferred_element_type=jnp.float32)
        up_part = jnp.dot(normed, up_weight[:, columns], preferred_element_type=jnp.float32)
        hidden = (jax.nn.silu(gate_part) * up_part).astype(jnp.bfloat16)
        partial_value = lax.dot_general(hidden, down_weight[:, columns], (((1,), (1,)), ((), ())), preferred_element_type=jnp.float32)
        feed_sum = feed_sum + lax.optimization_barrier(partial_value.astype(jnp.bfloat16)).astype(jnp.float32)
    return (stream + feed_sum).astype(jnp.bfloat16)
```

```python
import math

import jax
import jax.numpy as jnp
from jax import lax
from jax.experimental import pallas as pl
from jax.experimental.pallas import tpu as pltpu
from jax.sharding import PartitionSpec as P

epsilon = 1e-06


def map_update(state_in, queries, key_rows, value_block, score_scale):
    maxima, totals, accumulated = state_in
    scores = (
        jnp.einsum("thd,khd->htk", queries, key_rows, preferred_element_type=jnp.float32)
        * score_scale
    )
    newest = jnp.maximum(maxima, jnp.max(scores, axis=-1))
    factor = jnp.exp(maxima - newest)
    weights = jnp.exp(scores - newest[:, :, None])
    totals = totals * factor + jnp.sum(weights, axis=-1)
    product = jnp.einsum(
        "htk,khe->the",
        weights.astype(jnp.bfloat16),
        value_block,
        preferred_element_type=jnp.float32,
    )
    accumulated = accumulated * factor.T[:, :, None] + product
    return (newest, totals, accumulated)


def gathered_local(
    residual,
    query_first,
    key_first,
    query_second,
    key_second,
    values,
    lambda_weight,
    head_gain,
    out_weight,
    norm_gain,
    gate_weight,
    up_weight,
    down_weight,
):
    tokens_here = query_first.shape[0]
    head_count = lambda_weight.shape[0]
    head_size = query_first.shape[1] // head_count
    value_size = values.shape[1] // head_count
    score_scale = head_size ** (-0.5)
    queries_first = query_first.reshape(tokens_here, head_count, head_size)
    queries_second = query_second.reshape(tokens_here, head_count, head_size)
    empty_stats = (
        jnp.full((head_count, tokens_here), -jnp.inf, jnp.float32),
        jnp.zeros((head_count, tokens_here), jnp.float32),
        jnp.zeros((tokens_here, head_count, value_size), jnp.float32),
    )
    start_state = (empty_stats, empty_stats)
    keys_one = lax.all_gather(key_first, "sp", axis=0, tiled=True)
    row_count = keys_one.shape[0]
    block_rows = math.gcd(row_count, 1024)
    blocks = (
        keys_one.reshape(row_count // block_rows, block_rows, head_count, head_size),
        lax.all_gather(key_second, "sp", axis=0, tiled=True).reshape(
            row_count // block_rows, block_rows, head_count, head_size
        ),
        lax.all_gather(values, "sp", axis=0, tiled=True).reshape(
            row_count // block_rows, block_rows, head_count, value_size
        ),
    )

    def advance(current, block_keys):
        return (
            (
                map_update(current[0], queries_first, block_keys[0], block_keys[2], score_scale),
                map_update(current[1], queries_second, block_keys[1], block_keys[2], score_scale),
            ),
            None,
        )

    statistics = lax.scan(advance, start_state, blocks)[0]

    def finish(map_stats):
        return map_stats[2] / map_stats[1].T[:, :, None]

    difference = finish(statistics[0]) - lambda_weight[None, :, None] * finish(statistics[1])
    scaled = difference * lax.rsqrt(
        jnp.mean(difference * difference, axis=-1, keepdims=True) + epsilon
    )
    attended = (
        (scaled * head_gain).astype(jnp.bfloat16).reshape(tokens_here, head_count * value_size)
    )
    partial_value = lax.dot_general(
        attended,
        lax.all_gather(out_weight, "sp", axis=0, tiled=True),
        (((1,), (1,)), ((), ())),
        preferred_element_type=jnp.float32,
    )
    summed = lax.psum_scatter(
        partial_value.astype(jnp.bfloat16), "tp", scatter_dimension=0, tiled=True
    ).astype(jnp.float32)
    after_attention = (residual.astype(jnp.float32) + summed).astype(jnp.bfloat16)
    stream = after_attention.astype(jnp.float32)
    scaled_rows = stream * lax.rsqrt(jnp.mean(stream * stream, axis=-1, keepdims=True) + epsilon)
    shard_piece = lax.all_gather(
        (scaled_rows * norm_gain).astype(jnp.bfloat16), "tp", axis=0, tiled=True
    )
    gate_part = jnp.dot(shard_piece, gate_weight, preferred_element_type=jnp.float32)
    up_part = jnp.dot(shard_piece, up_weight, preferred_element_type=jnp.float32)
    hidden = (jax.nn.silu(gate_part) * up_part).astype(jnp.bfloat16)
    down_partial = lax.dot_general(
        hidden,
        lax.all_gather(down_weight, "sp", axis=0, tiled=True),
        (((1,), (1,)), ((), ())),
        preferred_element_type=jnp.float32,
    )
    feed_out = lax.psum_scatter(
        down_partial.astype(jnp.bfloat16), "tp", scatter_dimension=0, tiled=True
    ).astype(jnp.float32)
    return (after_attention.astype(jnp.float32) + feed_out).astype(jnp.bfloat16)


def attention_body(
    lambda_ref, gain_ref, q_ref, k0_ref, k1_ref, k32_ref, v0_ref, v3_ref, v12_ref, out_ref
):
    half_lanes = q_ref.shape[1] // 2
    rows = k0_ref.shape[0]
    heads = v0_ref.shape[1] // gain_ref.shape[1]
    head_size = half_lanes // heads
    value_size = gain_ref.shape[1]
    scale = head_size ** (-0.5)
    key_blocks = (
        (k0_ref, 0),
        (k1_ref, 0),
        (k32_ref, 0),
        (k32_ref, rows),
    )
    value_blocks = (
        (v0_ref, 0),
        (v12_ref, 0),
        (v3_ref, 0),
        (v12_ref, rows),
    )
    lane = lax.broadcasted_iota(jnp.int32, (q_ref.shape[0], half_lanes), 1)

    def one_map(head, which):
        q = q_ref[:, which * half_lanes : (which + 1) * half_lanes]
        q = jnp.where(
            (lane >= head * head_size) & (lane < (head + 1) * head_size), q, jnp.zeros_like(q)
        )
        scores = [
            lax.dot_general(
                q,
                ref[start : start + rows, which * half_lanes : (which + 1) * half_lanes],
                (((1,), (1,)), ((), ())),
                preferred_element_type=jnp.float32,
            )
            * scale
            for ref, start in key_blocks
        ]
        top = scores[0].max(axis=-1, keepdims=True)
        for block in scores[1:]:
            top = jnp.maximum(top, block.max(axis=-1, keepdims=True))
        total = None
        product = None
        for block, (ref, start) in zip(scores, value_blocks):
            shifted = jnp.exp(block - top)
            part = shifted.sum(axis=-1, keepdims=True)
            value = jnp.dot(
                shifted.astype(jnp.bfloat16),
                ref[start : start + rows, head * value_size : (head + 1) * value_size],
                preferred_element_type=jnp.float32,
            )
            total = part if total is None else total + part
            product = value if product is None else product + value
        return product / total

    for head in range(heads):
        difference = one_map(head, 0) - lambda_ref[head] * one_map(head, 1)
        scaled = difference * lax.rsqrt(
            jnp.mean(difference * difference, axis=-1, keepdims=True) + epsilon
        )
        out_ref[:, head * value_size : (head + 1) * value_size] = (
            scaled * gain_ref[...]
        ).astype(out_ref.dtype)


def attend(lambdas, gain, queries, key_parts, value_parts):
    vmem = pl.BlockSpec(memory_space=pltpu.VMEM)
    return pl.pallas_call(
        attention_body,
        out_shape=jax.ShapeDtypeStruct((queries.shape[0], value_parts[0].shape[1]), jnp.bfloat16),
        in_specs=[pl.BlockSpec(memory_space=pltpu.SMEM)] + [vmem] * 8,
        out_specs=vmem,
        name="attend",
    )(lambdas, gain.reshape(1, -1), queries, *key_parts, *value_parts)


def moved_local(
    sp_size,
    tp_size,
    residual,
    query_first,
    key_first,
    query_second,
    key_second,
    values,
    lambda_weight,
    head_gain,
    out_weight,
    norm_gain,
    gate_weight,
    up_weight,
    down_weight,
):
    side, near, far = 1, 2, sp_size - 2
    chip, core = tp_size // 2, 1
    both = ("sp", "tp")
    place = lax.axis_index("sp")
    member = lax.axis_index("tp")
    on_side = (place & 1) == 1

    def swap(array, axis, distance):
        count = sp_size if axis == "sp" else tp_size
        return lax.ppermute(array, axis, [(i, i ^ distance) for i in range(count)])

    def swap_both(array, first, second):
        pairs = [
            (i * tp_size + j, (i ^ first) * tp_size + (j ^ second))
            for i in range(sp_size)
            for j in range(tp_size)
        ]
        return lax.ppermute(array, both, pairs)

    tokens = query_first.shape[0]
    rows = tokens // tp_size
    width = residual.shape[1]

    def halves(array):
        middle = array.shape[1] // 2
        return array[:, :middle], array[:, middle:]

    def kept(array):
        left, right = halves(array)
        return jnp.where(on_side, right, left)

    def given(array):
        left, right = halves(array)
        return jnp.where(on_side, left, right)

    def by_distance(array):
        blocks = array.reshape(2, 2, rows, array.shape[1])
        blocks = jnp.where((member & 1) == 1, blocks[:, ::-1], blocks)
        blocks = jnp.where((member & 2) == 2, blocks[::-1], blocks)
        return blocks.reshape(array.shape)

    def spread(weight):
        middle = weight.shape[0] // 2
        first, second = weight[:middle], weight[middle:]
        first_near = swap(first, "sp", near)
        second_far = swap(second, "sp", far)
        first_two = jnp.concatenate([first, first_near], 0)
        second_two = jnp.concatenate([second, second_far], 0)
        first_rest = swap(first_two, "sp", far)
        second_rest = swap(second_two, "sp", near)
        return jnp.concatenate([first_two, first_rest, second_two, second_rest], 0)

    def scatter_sum(partial):
        sent = swap(partial[1].astype(jnp.bfloat16), "tp", core)
        ours = partial[0] + sent.astype(jnp.float32)
        rounded = ours.astype(jnp.bfloat16)
        from_chip = swap(rounded[0, 1], "tp", chip)
        from_side = swap(rounded[1, 0], "sp", side)
        from_both = swap_both(rounded[1, 1], side, chip)
        same = ours[0, 0] + from_chip.astype(jnp.float32)
        other = from_side.astype(jnp.float32) + from_both.astype(jnp.float32)
        left = jnp.where(on_side, other, same)
        right = jnp.where(on_side, same, other)
        piece = left.shape[1] // 8
        first_at = {0: 0, 1: 1, 3: 2, 2: 3}
        second_at = {0: 4, 3: 5, 1: 6, 2: 7}

        def block(array, k):
            a, b = first_at[k] * piece, second_at[k] * piece
            return [array[:, a : a + piece], array[:, b : b + piece]]

        near_blocks = [
            jnp.concatenate(block(left, k) + block(right, k), axis=1) for k in range(4)
        ]
        low = (place & 2) == 2
        high = (place & 4) == 4
        n = [jnp.where(low, near_blocks[k ^ 1], near_blocks[k]) for k in range(4)]
        n = [jnp.where(high, n[k ^ 2], n[k]) for k in range(4)]
        return jnp.concatenate(n, axis=1)

    queries = [by_distance(query_first), by_distance(query_second)]
    sent = jnp.concatenate(
        [given(a) for a in (*queries, key_first, key_second, values)], axis=1
    )
    mine = [kept(a) for a in (*queries, key_first, key_second, values)]
    got = swap(sent, "sp", side)
    lanes = mine[0].shape[1]
    query_rows = jnp.concatenate(
        [jnp.concatenate(mine[:2], axis=1), got[:, : 2 * lanes]], axis=0
    )
    key_rows = jnp.concatenate(
        [jnp.concatenate(mine[2:4], axis=1), got[:, 2 * lanes : 4 * lanes]], axis=0
    )
    value_rows = jnp.concatenate([mine[4], got[:, 4 * lanes :]], axis=0)
    key_near = swap(key_rows, "sp", near)
    value_far = swap(value_rows, "sp", far)
    key_rest = swap(jnp.concatenate([key_rows, key_near], 0), "sp", far)
    value_rest = swap(jnp.concatenate([value_rows, value_far], 0), "sp", near)
    middle = lambda_weight.shape[0] // 2
    lambdas = jnp.where(on_side, lambda_weight[middle:], lambda_weight[:middle])
    attended = attend(
        lambdas,
        head_gain,
        query_rows,
        (key_rows, key_near, key_rest),
        (value_rows, value_far, value_rest),
    )

    out_rows = spread(jnp.concatenate([kept(out_weight), given(out_weight)], axis=1))
    other_heads = swap(attended, "sp", side)
    other_heads = jnp.concatenate([other_heads[tokens:], other_heads[:tokens]], 0)
    projected = lax.dot_general(
        jnp.concatenate([attended, other_heads], axis=1),
        out_rows,
        (((1,), (1,)), ((), ())),
        preferred_element_type=jnp.float32,
    ).reshape(2, 2, 2, rows, width // 2)
    summed = scatter_sum(projected.transpose(2, 0, 1, 3, 4))
    after_attention = (residual.astype(jnp.float32) + summed).astype(jnp.bfloat16)
    stream = after_attention.astype(jnp.float32)
    scaled_rows = stream * lax.rsqrt(jnp.mean(stream * stream, axis=-1, keepdims=True) + epsilon)
    normed = (scaled_rows * norm_gain).astype(jnp.bfloat16)

    four = jnp.concatenate(
        [
            normed,
            swap(normed, "tp", chip),
            swap(normed, "sp", side),
            swap_both(normed, side, chip),
        ],
        axis=0,
    )
    eight = jnp.concatenate([four, swap(four, "tp", core)], axis=0)
    gate_part = jnp.dot(eight, gate_weight, preferred_element_type=jnp.float32)
    up_part = jnp.dot(eight, up_weight, preferred_element_type=jnp.float32)
    hidden = (jax.nn.silu(gate_part) * up_part).astype(jnp.bfloat16)
    down_partial = lax.dot_general(
        hidden,
        spread(down_weight),
        (((1,), (1,)), ((), ())),
        preferred_element_type=jnp.float32,
    ).reshape(2, 2, 2, rows, width // 2)
    return (stream + scatter_sum(down_partial)).astype(jnp.bfloat16)


def solution(mesh):
    sp_size, tp_size = mesh.shape["sp"], mesh.shape["tp"]

    def local(*arrays):
        total_tokens = arrays[1].shape[0] * sp_size
        short = total_tokens <= arrays[0].shape[1]
        if short and (sp_size, tp_size) == (8, 4):
            return moved_local(sp_size, tp_size, *arrays)
        return gathered_local(*arrays)

    return jax.shard_map(
        local,
        mesh=mesh,
        in_specs=(
            P(("sp", "tp"), None),
            P("sp", "tp"),
            P("sp", "tp"),
            P("sp", "tp"),
            P("sp", "tp"),
            P("sp", "tp"),
            P("tp"),
            P(),
            P("sp", "tp"),
            P(),
            P(None, "tp"),
            P(None, "tp"),
            P("sp", "tp"),
        ),
        out_specs=P(("sp", "tp"), None),
        check_vma=False,
    )
```

```python
import functools
import math

import jax
import jax.numpy as jnp
from jax import lax
from jax.experimental import pallas as pl
from jax.experimental.pallas import tpu as pltpu
from jax.sharding import PartitionSpec as P


epsilon = 1e-06


def map_update(state_in, queries, key_rows, value_block, score_scale):
    maxima, totals, accumulated = state_in
    scores = (
        jnp.einsum("thd,khd->htk", queries, key_rows, preferred_element_type=jnp.float32)
        * score_scale
    )
    newest = jnp.maximum(maxima, jnp.max(scores, axis=-1))
    factor = jnp.exp(maxima - newest)
    weights = jnp.exp(scores - newest[:, :, None])
    totals = totals * factor + jnp.sum(weights, axis=-1)
    product = jnp.einsum(
        "htk,khe->the",
        weights.astype(jnp.bfloat16),
        value_block,
        preferred_element_type=jnp.float32,
    )
    accumulated = accumulated * factor.T[:, :, None] + product
    return (newest, totals, accumulated)


def gathered_local(
    residual,
    query_first,
    key_first,
    query_second,
    key_second,
    values,
    lambda_weight,
    head_gain,
    out_weight,
    norm_gain,
    gate_weight,
    up_weight,
    down_weight,
):
    tokens_here = query_first.shape[0]
    head_count = lambda_weight.shape[0]
    head_size = query_first.shape[1] // head_count
    value_size = values.shape[1] // head_count
    score_scale = head_size ** (-0.5)
    queries_first = query_first.reshape(tokens_here, head_count, head_size)
    queries_second = query_second.reshape(tokens_here, head_count, head_size)
    empty_stats = (
        jnp.full((head_count, tokens_here), -jnp.inf, jnp.float32),
        jnp.zeros((head_count, tokens_here), jnp.float32),
        jnp.zeros((tokens_here, head_count, value_size), jnp.float32),
    )
    start_state = (empty_stats, empty_stats)
    keys_one = lax.all_gather(key_first, "sp", axis=0, tiled=True)
    row_count = keys_one.shape[0]
    block_rows = math.gcd(row_count, 1024)
    blocks = (
        keys_one.reshape(row_count // block_rows, block_rows, head_count, head_size),
        lax.all_gather(key_second, "sp", axis=0, tiled=True).reshape(
            row_count // block_rows, block_rows, head_count, head_size
        ),
        lax.all_gather(values, "sp", axis=0, tiled=True).reshape(
            row_count // block_rows, block_rows, head_count, value_size
        ),
    )

    def advance(current, block_keys):
        return (
            (
                map_update(current[0], queries_first, block_keys[0], block_keys[2], score_scale),
                map_update(current[1], queries_second, block_keys[1], block_keys[2], score_scale),
            ),
            None,
        )

    statistics = lax.scan(advance, start_state, blocks)[0]

    def finish(map_stats):
        return map_stats[2] / map_stats[1].T[:, :, None]

    difference = finish(statistics[0]) - lambda_weight[None, :, None] * finish(statistics[1])
    scaled = difference * lax.rsqrt(
        jnp.mean(difference * difference, axis=-1, keepdims=True) + epsilon
    )
    attended = (
        (scaled * head_gain).astype(jnp.bfloat16).reshape(tokens_here, head_count * value_size)
    )
    partial_value = lax.dot_general(
        attended,
        lax.all_gather(out_weight, "sp", axis=0, tiled=True),
        (((1,), (1,)), ((), ())),
        preferred_element_type=jnp.float32,
    )
    summed = lax.psum_scatter(
        partial_value.astype(jnp.bfloat16), "tp", scatter_dimension=0, tiled=True
    ).astype(jnp.float32)
    after_attention = (residual.astype(jnp.float32) + summed).astype(jnp.bfloat16)
    stream = after_attention.astype(jnp.float32)
    scaled_rows = stream * lax.rsqrt(jnp.mean(stream * stream, axis=-1, keepdims=True) + epsilon)
    shard_piece = lax.all_gather(
        (scaled_rows * norm_gain).astype(jnp.bfloat16), "tp", axis=0, tiled=True
    )
    gate_part = jnp.dot(shard_piece, gate_weight, preferred_element_type=jnp.float32)
    up_part = jnp.dot(shard_piece, up_weight, preferred_element_type=jnp.float32)
    hidden = (jax.nn.silu(gate_part) * up_part).astype(jnp.bfloat16)
    down_partial = lax.dot_general(
        hidden,
        lax.all_gather(down_weight, "sp", axis=0, tiled=True),
        (((1,), (1,)), ((), ())),
        preferred_element_type=jnp.float32,
    )
    feed_out = lax.psum_scatter(
        down_partial.astype(jnp.bfloat16), "tp", scatter_dimension=0, tiled=True
    ).astype(jnp.float32)
    return (after_attention.astype(jnp.float32) + feed_out).astype(jnp.bfloat16)


def deal_body(*refs, sp_size, tp_size):
    sources, out_ref, extra_ref, arrived, sems = refs[:7], refs[7], refs[8], refs[9:16], refs[16]
    copies = [
        pltpu.make_async_copy(source, to, sems.at[index])
        for index, (source, to) in enumerate(zip(sources, arrived))
    ]
    for copy in copies:
        copy.start()
    for copy in copies:
        copy.wait()
    qf_ref, kf_ref, qs_ref, ks_ref, v_ref, gain_ref, lambda_ref = arrived
    here = lax.axis_index("sp") // 2
    member = lax.axis_index("tp")
    heads = sp_size // 2
    rows = qf_ref.shape[0] // tp_size
    size = qf_ref.shape[1] // heads
    value_size = v_ref.shape[1] // heads
    extra_ref[0:1] = gain_ref[...]
    extra_ref[1:2] = jnp.full((1, value_size), lambda_ref[here], jnp.float32)
    for block in range(tp_size):
        at = pl.ds(pl.multiple_of((member ^ block) * rows, rows), rows)
        for head in range(heads):
            columns = slice(head * size, (head + 1) * size)
            narrow = [ref[at, columns] for ref in (qf_ref, qs_ref, kf_ref, ks_ref)]
            out_ref[here ^ head, block * rows : (block + 1) * rows, :] = jnp.concatenate(
                narrow + [v_ref[at, head * value_size : (head + 1) * value_size]], axis=1
            )


def attention_body(
    extra_ref, a_ref, b_ref, c_ref, d_ref, ab_ref, cd_ref, out_ref, k_ref, v_ref
):
    rows = a_ref.shape[0]
    gain, weight = extra_ref[0:1], extra_ref[1:2]
    lanes = a_ref.shape[1] - ab_ref.shape[1]
    head_size = lanes // 2
    scale = head_size ** (-0.5)
    queries = (a_ref, b_ref, c_ref, d_ref)
    for index, ref in enumerate(queries):
        k_ref[index * rows : (index + 1) * rows] = ref[:, lanes : 2 * lanes]
        v_ref[index * rows : (index + 1) * rows] = ref[:, 2 * lanes :]
    for index, ref in enumerate((ab_ref, cd_ref)):
        at = slice((4 + 2 * index) * rows, (6 + 2 * index) * rows)
        k_ref[at] = ref[:, :lanes]
        v_ref[at] = ref[:, lanes:]
    lane = lax.broadcasted_iota(jnp.int32, (rows, lanes), 1)

    def one_map(query, which):
        wanted = (lane < head_size) if which == 0 else (lane >= head_size)
        scores = (
            lax.dot_general(
                jnp.where(wanted, query, jnp.zeros_like(query)),
                k_ref[...],
                (((1,), (1,)), ((), ())),
                preferred_element_type=jnp.float32,
            )
            * scale
        )
        shifted = jnp.exp(scores - scores.max(axis=-1, keepdims=True))
        total = shifted.sum(axis=-1, keepdims=True)
        product = jnp.dot(
            shifted.astype(jnp.bfloat16), v_ref[...], preferred_element_type=jnp.float32
        )
        return product / total

    for index, ref in enumerate(queries):
        query = ref[:, :lanes]
        difference = one_map(query, 0) - weight * one_map(query, 1)
        scaled = difference * lax.rsqrt(
            jnp.mean(difference * difference, axis=-1, keepdims=True) + epsilon
        )
        out_ref[index] = (scaled * gain).astype(out_ref.dtype)


def project_body(
    own_ref, other_ref, b_ref, c_ref, d_ref, source, kept_ref, sent_ref, a_ref, sem, *, tp_size
):
    copy = pltpu.make_async_copy(source, a_ref, sem)
    copy.start()
    rows = own_ref.shape[0] // tp_size
    width = a_ref.shape[0]
    for index, ref in ((1, b_ref), (2, c_ref), (3, d_ref), (0, a_ref)):
        if index == 0:
            copy.wait()
        columns = slice(index * width, (index + 1) * width)
        for side, left_ref in enumerate((own_ref, other_ref)):
            product = lax.dot_general(
                left_ref[...], ref[...], (((1,), (1,)), ((), ())), preferred_element_type=jnp.float32
            )
            for chip in range(tp_size // 2):
                to = slice((side * 2 + chip) * rows, (side * 2 + chip + 1) * rows)
                at = chip * 2 * rows
                kept_ref[to, columns] = product[at : at + rows]
                sent_ref[to, columns] = product[at + rows : at + 2 * rows].astype(sent_ref.dtype)


def gate_body(here_ref, there_ref, gate_ref, up_ref, hidden_ref, both_ref, *rest, tile):
    rows = here_ref.shape[0]
    units = gate_ref.shape[1]
    starts = range(0, units, tile)
    buffers, sems = rest[:-1], rest[-1]
    copies = []
    for index, start in enumerate(starts):
        columns = pl.ds(start, min(tile, units - start))
        pair = [
            pltpu.make_async_copy(
                ref.at[:, columns], buffers[2 * index + which], sems.at[2 * index + which]
            )
            for which, ref in enumerate((gate_ref, up_ref))
        ]
        for copy in pair:
            copy.start()
        copies.append(pair)
    both_ref[:rows] = here_ref[...]
    both_ref[rows:] = there_ref[...]
    for index, start in enumerate(starts):
        for copy in copies[index]:
            copy.wait()
        gate, up = (
            jnp.dot(
                both_ref[...], buffers[2 * index + which][...], preferred_element_type=jnp.float32
            )
            for which in range(2)
        )
        hidden = gate / (1.0 + jnp.exp(-gate)) * up
        hidden_ref[:, start : start + gate.shape[1]] = hidden.astype(hidden_ref.dtype)


def down_body(
    hidden_ref,
    own_ref,
    near_ref,
    third_inner_ref,
    third_outer_ref,
    last_inner_ref,
    last_outer_ref,
    kept_ref,
    sent_ref,
    *,
    sp_size,
):
    place = lax.axis_index("sp") // 2
    inner = (place > 0) & (place < sp_size // 2 - 1)
    rows = kept_ref.shape[0]
    width = own_ref.shape[0]
    pieces = (
        own_ref[...],
        near_ref[...],
        jnp.where(inner, third_inner_ref[...], third_outer_ref[...]),
        jnp.where(inner, last_inner_ref[...], last_outer_ref[...]),
    )
    for index, piece in enumerate(pieces):
        product = lax.dot_general(
            hidden_ref[...], piece, (((1,), (1,)), ((), ())), preferred_element_type=jnp.float32
        )
        columns = slice(index * width, (index + 1) * width)
        kept_ref[:, columns] = product[:rows]
        sent_ref[:, columns] = product[rows:].astype(sent_ref.dtype)


def kernel(body, out_shape, near, away=(), scratch=(), limit=16):
    vmem = pl.BlockSpec(memory_space=pltpu.VMEM)
    many = isinstance(out_shape, tuple)
    call = pl.pallas_call(
        body,
        out_shape=out_shape,
        in_specs=[vmem] * len(near) + [pl.BlockSpec(memory_space=pltpu.HBM)] * len(away),
        out_specs=(vmem,) * len(out_shape) if many else vmem,
        scratch_shapes=list(scratch),
        compiler_params=pltpu.CompilerParams(vmem_limit_bytes=limit * 2**20),
    )
    return call(*near, *(pltpu.with_memory_space_constraint(array, pltpu.HBM) for array in away))


def moved_local(
    sp_size,
    tp_size,
    residual,
    query_first,
    key_first,
    query_second,
    key_second,
    values,
    lambda_weight,
    head_gain,
    out_weight,
    norm_gain,
    gate_weight,
    up_weight,
    down_weight,
):
    side, near, across, far = 1, 2, sp_size // 2, sp_size - 2
    planes = sp_size // 2
    chip, core = tp_size // 2, 1
    place = lax.axis_index("sp")
    on_side = (place & 1) == 1
    low = (place & 2) == 2
    high = (place & 4) == 4
    bf16, f32 = jnp.bfloat16, jnp.float32

    def swap(array, axis, distance):
        count = sp_size if axis == "sp" else tp_size
        return lax.ppermute(array, axis, [(i, i ^ distance) for i in range(count)])

    def swap_both(array, first, second):
        pairs = [
            (i * tp_size + j, (i ^ first) * tp_size + (j ^ second))
            for i in range(sp_size)
            for j in range(tp_size)
        ]
        return lax.ppermute(array, ("sp", "tp"), pairs)

    inner = [i for i in range(sp_size) if 0 < i // 2 < planes - 1]
    middle_pairs = [(i, i ^ far) for i in inner]
    outward_pairs = [(i, i ^ near) for i in inner]

    def three(first, second, third):
        third = swap(third, "sp", far)
        second = swap(second, "sp", across)
        return swap(first, "sp", near), second, third

    def along_line(weight):
        near_one = swap(weight, "sp", near)
        middle_one = lax.ppermute(weight, "sp", middle_pairs)
        middle_two = lax.ppermute(near_one, "sp", middle_pairs)
        outer_one = lax.ppermute(middle_one, "sp", outward_pairs)
        outer_two = lax.ppermute(middle_two, "sp", outward_pairs)
        return weight, near_one, middle_one, outer_one, middle_two, outer_two

    def planes_by_distance(n):
        n = [jnp.where(low, n[k ^ 1], n[k]) for k in range(4)]
        return [jnp.where(high, n[k ^ 2], n[k]) for k in range(4)]

    def planes_along_line(n):
        first, second = jnp.where(low, n[1], n[0]), jnp.where(low, n[0], n[1])
        return [
            jnp.where(high, n[3], first),
            jnp.where(high, n[2], second),
            jnp.where(high, first, n[2]),
            jnp.where(high, second, n[3]),
        ]

    def scatter_sum(ours, given_away, ordered):
        ours = ours + swap(given_away, "tp", core).astype(f32)
        rows = ours.shape[0] // 4
        rounded = ours.astype(bf16)
        from_both = swap_both(rounded[3 * rows :], side, chip)
        from_side = swap(rounded[2 * rows : 3 * rows], "sp", side)
        from_chip = swap(rounded[rows : 2 * rows], "tp", chip)
        same = ours[:rows] + from_chip.astype(f32)
        other = from_side.astype(f32) + from_both.astype(f32)
        piece = same.shape[1] // planes
        joined = []
        for k in range(planes):
            a, b = (array[:, k * piece : (k + 1) * piece] for array in (same, other))
            joined.append(
                jnp.concatenate([jnp.where(on_side, b, a), jnp.where(on_side, a, b)], axis=1)
            )
        return jnp.concatenate(ordered(joined), axis=1)

    tokens = query_first.shape[0]
    rows = tokens // tp_size
    head_lanes = 2 * query_first.shape[1] // planes
    value_size = head_gain.shape[0]

    streams = (query_first, key_first, query_second, key_second, values)
    dealt, extra = kernel(
        functools.partial(deal_body, sp_size=sp_size, tp_size=tp_size),
        (
            jax.ShapeDtypeStruct((planes, tokens, 2 * head_lanes + value_size), bf16),
            jax.ShapeDtypeStruct((2, value_size), f32),
        ),
        (),
        (*streams, head_gain.reshape(1, -1), lambda_weight),
        [pltpu.VMEM(array.shape, bf16) for array in streams]
        + [
            pltpu.VMEM((1, value_size), f32),
            pltpu.SMEM(lambda_weight.shape, f32),
            pltpu.SemaphoreType.DMA((7,)),
        ],
    )
    first, second, third = three(dealt[1], dealt[2], dealt[3])
    early = swap(jnp.concatenate([dealt[0][:, head_lanes:], first[:, head_lanes:]], 0), "sp", side)
    late = swap(jnp.concatenate([second[:, head_lanes:], third[:, head_lanes:]], 0), "sp", side)
    attended = kernel(
        attention_body,
        jax.ShapeDtypeStruct((planes, tokens, value_size), bf16),
        (extra, dealt[0], first, second, third, early, late),
        scratch=[
            pltpu.VMEM((2 * planes * tokens, head_lanes), bf16),
            pltpu.VMEM((2 * planes * tokens, value_size), bf16),
        ],
    )
    back = three(attended[1], attended[2], attended[3])
    own_heads = jnp.concatenate(planes_by_distance([attended[0], *back]), axis=1)
    other_heads = swap(own_heads, "sp", side)

    half = (4 * rows, residual.shape[1] // 2)
    halves = (jax.ShapeDtypeStruct(half, f32), jax.ShapeDtypeStruct(half, bf16))
    projected = kernel(
        functools.partial(project_body, tp_size=tp_size),
        halves,
        (own_heads, other_heads, *three(out_weight, out_weight, out_weight)),
        (out_weight,),
        [pltpu.VMEM(out_weight.shape, bf16), pltpu.SemaphoreType.DMA],
    )
    summed = scatter_sum(*projected, planes_by_distance)
    after_attention = (residual.astype(f32) + summed).astype(bf16)
    stream = after_attention.astype(f32)
    scaled_rows = stream * lax.rsqrt(jnp.mean(stream * stream, axis=-1, keepdims=True) + epsilon)
    normed = (scaled_rows * norm_gain).astype(bf16)

    from_both = swap_both(normed, side, chip)
    from_side = swap(normed, "sp", side)
    from_chip = swap(normed, "tp", chip)
    four = jnp.concatenate([normed, from_chip, from_side, from_both], axis=0)
    units = gate_weight.shape[1]
    tile = 256
    sizes = [min(tile, units - start) for start in range(0, units, tile) for _ in range(2)]
    hidden = kernel(
        functools.partial(gate_body, tile=tile),
        jax.ShapeDtypeStruct((8 * rows, units), bf16),
        (four, swap(four, "tp", core)),
        (gate_weight, up_weight),
        [pltpu.VMEM((8 * rows, residual.shape[1]), bf16)]
        + [pltpu.VMEM((residual.shape[1], size), bf16) for size in sizes]
        + [pltpu.SemaphoreType.DMA((len(sizes),))],
        limit=24,
    )
    fed = kernel(
        functools.partial(down_body, sp_size=sp_size), halves, (hidden, *along_line(down_weight))
    )
    return (stream + scatter_sum(*fed, planes_along_line)).astype(bf16)


def solution(mesh):
    sp_size, tp_size = mesh.shape["sp"], mesh.shape["tp"]

    def local(*arrays):
        total_tokens = arrays[1].shape[0] * sp_size
        short = total_tokens <= arrays[0].shape[1]
        if short and (sp_size, tp_size) == (8, 4):
            return moved_local(sp_size, tp_size, *arrays)
        return gathered_local(*arrays)

    return jax.shard_map(
        local,
        mesh=mesh,
        in_specs=(
            P(("sp", "tp"), None),
            P("sp", "tp"),
            P("sp", "tp"),
            P("sp", "tp"),
            P("sp", "tp"),
            P("sp", "tp"),
            P("tp"),
            P(),
            P("sp", "tp"),
            P(),
            P(None, "tp"),
            P(None, "tp"),
            P("sp", "tp"),
        ),
        out_specs=P(("sp", "tp"), None),
        check_vma=False,
    )
```

```python
import functools
import math

import jax
import jax.numpy as jnp
from jax import lax
from jax.experimental import pallas as pl
from jax.experimental.pallas import tpu as pltpu
from jax.sharding import PartitionSpec as P


epsilon = 1e-06


def map_update(state_in, queries, key_rows, value_block, score_scale):
    maxima, totals, accumulated = state_in
    scores = (
        jnp.einsum("thd,khd->htk", queries, key_rows, preferred_element_type=jnp.float32)
        * score_scale
    )
    newest = jnp.maximum(maxima, jnp.max(scores, axis=-1))
    factor = jnp.exp(maxima - newest)
    weights = jnp.exp(scores - newest[:, :, None])
    totals = totals * factor + jnp.sum(weights, axis=-1)
    product = jnp.einsum(
        "htk,khe->the",
        weights.astype(jnp.bfloat16),
        value_block,
        preferred_element_type=jnp.float32,
    )
    accumulated = accumulated * factor.T[:, :, None] + product
    return (newest, totals, accumulated)


def gathered_local(
    residual,
    query_first,
    key_first,
    query_second,
    key_second,
    values,
    lambda_weight,
    head_gain,
    out_weight,
    norm_gain,
    gate_weight,
    up_weight,
    down_weight,
):
    tokens_here = query_first.shape[0]
    head_count = lambda_weight.shape[0]
    head_size = query_first.shape[1] // head_count
    value_size = values.shape[1] // head_count
    score_scale = head_size ** (-0.5)
    queries_first = query_first.reshape(tokens_here, head_count, head_size)
    queries_second = query_second.reshape(tokens_here, head_count, head_size)
    empty_stats = (
        jnp.full((head_count, tokens_here), -jnp.inf, jnp.float32),
        jnp.zeros((head_count, tokens_here), jnp.float32),
        jnp.zeros((tokens_here, head_count, value_size), jnp.float32),
    )
    start_state = (empty_stats, empty_stats)
    keys_one = lax.all_gather(key_first, "sp", axis=0, tiled=True)
    row_count = keys_one.shape[0]
    block_rows = math.gcd(row_count, 1024)
    blocks = (
        keys_one.reshape(row_count // block_rows, block_rows, head_count, head_size),
        lax.all_gather(key_second, "sp", axis=0, tiled=True).reshape(
            row_count // block_rows, block_rows, head_count, head_size
        ),
        lax.all_gather(values, "sp", axis=0, tiled=True).reshape(
            row_count // block_rows, block_rows, head_count, value_size
        ),
    )

    def advance(current, block_keys):
        return (
            (
                map_update(current[0], queries_first, block_keys[0], block_keys[2], score_scale),
                map_update(current[1], queries_second, block_keys[1], block_keys[2], score_scale),
            ),
            None,
        )

    statistics = lax.scan(advance, start_state, blocks)[0]

    def finish(map_stats):
        return map_stats[2] / map_stats[1].T[:, :, None]

    difference = finish(statistics[0]) - lambda_weight[None, :, None] * finish(statistics[1])
    scaled = difference * lax.rsqrt(
        jnp.mean(difference * difference, axis=-1, keepdims=True) + epsilon
    )
    attended = (
        (scaled * head_gain).astype(jnp.bfloat16).reshape(tokens_here, head_count * value_size)
    )
    partial_value = lax.dot_general(
        attended,
        lax.all_gather(out_weight, "sp", axis=0, tiled=True),
        (((1,), (1,)), ((), ())),
        preferred_element_type=jnp.float32,
    )
    summed = lax.psum_scatter(
        partial_value.astype(jnp.bfloat16), "tp", scatter_dimension=0, tiled=True
    ).astype(jnp.float32)
    after_attention = (residual.astype(jnp.float32) + summed).astype(jnp.bfloat16)
    stream = after_attention.astype(jnp.float32)
    scaled_rows = stream * lax.rsqrt(jnp.mean(stream * stream, axis=-1, keepdims=True) + epsilon)
    shard_piece = lax.all_gather(
        (scaled_rows * norm_gain).astype(jnp.bfloat16), "tp", axis=0, tiled=True
    )
    gate_part = jnp.dot(shard_piece, gate_weight, preferred_element_type=jnp.float32)
    up_part = jnp.dot(shard_piece, up_weight, preferred_element_type=jnp.float32)
    hidden = (jax.nn.silu(gate_part) * up_part).astype(jnp.bfloat16)
    down_partial = lax.dot_general(
        hidden,
        lax.all_gather(down_weight, "sp", axis=0, tiled=True),
        (((1,), (1,)), ((), ())),
        preferred_element_type=jnp.float32,
    )
    feed_out = lax.psum_scatter(
        down_partial.astype(jnp.bfloat16), "tp", scatter_dimension=0, tiled=True
    ).astype(jnp.float32)
    return (after_attention.astype(jnp.float32) + feed_out).astype(jnp.bfloat16)


def deal_body(*refs, sp_size, tp_size):
    sources, out_ref, extra_ref, arrived, sems = refs[:7], refs[7], refs[8], refs[9:16], refs[16]
    copies = [
        pltpu.make_async_copy(source, to, sems.at[index])
        for index, (source, to) in enumerate(zip(sources, arrived))
    ]
    for copy in copies:
        copy.start()
    for copy in copies:
        copy.wait()
    qf_ref, kf_ref, qs_ref, ks_ref, v_ref, gain_ref, lambda_ref = arrived
    here = lax.axis_index("sp") // 2
    member = lax.axis_index("tp")
    heads = sp_size // 2
    rows = qf_ref.shape[0] // tp_size
    size = qf_ref.shape[1] // heads
    value_size = v_ref.shape[1] // heads
    extra_ref[0:1] = gain_ref[...]
    extra_ref[1:2] = jnp.full((1, value_size), lambda_ref[here], jnp.float32)
    for block in range(tp_size):
        at = pl.ds(pl.multiple_of((member ^ block) * rows, rows), rows)
        for head in range(heads):
            columns = slice(head * size, (head + 1) * size)
            narrow = [ref[at, columns] for ref in (qf_ref, qs_ref, kf_ref, ks_ref)]
            out_ref[here ^ head, block * rows : (block + 1) * rows, :] = jnp.concatenate(
                narrow + [v_ref[at, head * value_size : (head + 1) * value_size]], axis=1
            )


def attention_body(
    extra_ref, a_ref, b_ref, c_ref, d_ref, ab_ref, cd_ref, out_ref, k_ref, v_ref
):
    rows = a_ref.shape[0]
    gain, weight = extra_ref[0:1], extra_ref[1:2]
    lanes = a_ref.shape[1] - ab_ref.shape[1]
    head_size = lanes // 2
    scale = head_size ** (-0.5)
    queries = (a_ref, b_ref, c_ref, d_ref)
    for index, ref in enumerate(queries):
        k_ref[index * rows : (index + 1) * rows] = ref[:, lanes : 2 * lanes]
        v_ref[index * rows : (index + 1) * rows] = ref[:, 2 * lanes :]
    for index, ref in enumerate((ab_ref, cd_ref)):
        at = slice((4 + 2 * index) * rows, (6 + 2 * index) * rows)
        k_ref[at] = ref[:, :lanes]
        v_ref[at] = ref[:, lanes:]
    lane = lax.broadcasted_iota(jnp.int32, (rows, lanes), 1)

    def one_map(query, which):
        wanted = (lane < head_size) if which == 0 else (lane >= head_size)
        scores = (
            lax.dot_general(
                jnp.where(wanted, query, jnp.zeros_like(query)),
                k_ref[...],
                (((1,), (1,)), ((), ())),
                preferred_element_type=jnp.float32,
            )
            * scale
        )
        shifted = jnp.exp(scores - scores.max(axis=-1, keepdims=True))
        total = shifted.sum(axis=-1, keepdims=True)
        product = jnp.dot(
            shifted.astype(jnp.bfloat16), v_ref[...], preferred_element_type=jnp.float32
        )
        return product / total

    for index, ref in enumerate(queries):
        query = ref[:, :lanes]
        difference = one_map(query, 0) - weight * one_map(query, 1)
        scaled = difference * lax.rsqrt(
            jnp.mean(difference * difference, axis=-1, keepdims=True) + epsilon
        )
        out_ref[index] = (scaled * gain).astype(out_ref.dtype)


def project_body(
    a_ref, b_ref, c_ref, d_ref, other_ref, source, kept_ref, sent_ref, own_ref, heads_ref, sem, *, tp_size
):
    copy = pltpu.make_async_copy(source, own_ref, sem)
    copy.start()
    here = lax.axis_index("sp") // 2
    planes, tokens, size = a_ref.shape
    for distance, ref in enumerate((a_ref, b_ref, c_ref, d_ref)):
        columns = pl.ds(pl.multiple_of((here ^ distance) * size, size), size)
        for block in range(planes):
            heads_ref[block * tokens : (block + 1) * tokens, columns] = ref[distance ^ block]
    rows = tokens // tp_size
    width = own_ref.shape[0]
    for index, ref in ((1, other_ref), (0, own_ref)):
        if index == 0:
            copy.wait()
        columns = slice(index * width, (index + 1) * width)
        product = lax.dot_general(
            heads_ref[...], ref[...], (((1,), (1,)), ((), ())), preferred_element_type=jnp.float32
        )
        for block in range(planes):
            for chip in range(tp_size // 2):
                to = slice((chip * planes + block) * rows, (chip * planes + block + 1) * rows)
                at = block * tokens + chip * 2 * rows
                kept_ref[to, columns] = product[at : at + rows]
                sent_ref[to, columns] = product[at + rows : at + 2 * rows].astype(sent_ref.dtype)


def gate_body(here_ref, there_ref, gate_ref, up_ref, hidden_ref, both_ref, *rest, tile):
    rows = here_ref.shape[0]
    units = gate_ref.shape[1]
    starts = range(0, units, tile)
    buffers, sems = rest[:-1], rest[-1]
    copies = []
    for index, start in enumerate(starts):
        columns = pl.ds(start, min(tile, units - start))
        pair = [
            pltpu.make_async_copy(
                ref.at[:, columns], buffers[2 * index + which], sems.at[2 * index + which]
            )
            for which, ref in enumerate((gate_ref, up_ref))
        ]
        for copy in pair:
            copy.start()
        copies.append(pair)
    both_ref[:rows] = here_ref[...]
    both_ref[rows:] = there_ref[...]
    for index, start in enumerate(starts):
        for copy in copies[index]:
            copy.wait()
        gate, up = (
            jnp.dot(
                both_ref[...], buffers[2 * index + which][...], preferred_element_type=jnp.float32
            )
            for which in range(2)
        )
        hidden = gate / (1.0 + jnp.exp(-gate)) * up
        hidden_ref[:, start : start + gate.shape[1]] = hidden.astype(hidden_ref.dtype)


def down_body(hidden_ref, own_ref, *refs, sp_size):
    parts, (kept_ref, sent_ref) = refs[:-2], refs[-2:]
    parts = [parts[start : start + 5] for start in range(0, len(parts), 5)]
    place = lax.axis_index("sp") // 2
    inner = (place > 0) & (place < sp_size // 2 - 1)
    rows = kept_ref.shape[0]
    width = own_ref.shape[0]

    def third(part):
        return jnp.where(inner, part[1][...], part[2][...])

    def last(part):
        return jnp.where(inner, part[3][...], part[4][...])

    pieces = (
        lambda: own_ref[...],
        lambda: jnp.concatenate([part[0][...] for part in parts], axis=0),
        lambda: jnp.concatenate([third(part) for part in parts], axis=0),
        lambda: jnp.concatenate([last(part) for part in parts], axis=0),
    )
    for index, piece in enumerate(pieces):
        product = lax.dot_general(
            hidden_ref[...], piece(), (((1,), (1,)), ((), ())), preferred_element_type=jnp.float32
        )
        columns = slice(index * width, (index + 1) * width)
        kept_ref[:, columns] = product[:rows]
        sent_ref[:, columns] = product[rows:].astype(sent_ref.dtype)


def kernel(body, out_shape, near, away=(), scratch=(), limit=16):
    vmem = pl.BlockSpec(memory_space=pltpu.VMEM)
    many = isinstance(out_shape, tuple)
    call = pl.pallas_call(
        body,
        out_shape=out_shape,
        in_specs=[vmem] * len(near) + [pl.BlockSpec(memory_space=pltpu.HBM)] * len(away),
        out_specs=(vmem,) * len(out_shape) if many else vmem,
        scratch_shapes=list(scratch),
        compiler_params=pltpu.CompilerParams(vmem_limit_bytes=limit * 2**20),
    )
    return call(*near, *(pltpu.with_memory_space_constraint(array, pltpu.HBM) for array in away))


def moved_local(
    sp_size,
    tp_size,
    residual,
    query_first,
    key_first,
    query_second,
    key_second,
    values,
    lambda_weight,
    head_gain,
    out_weight,
    norm_gain,
    gate_weight,
    up_weight,
    down_weight,
):
    side, near, across, far = 1, 2, sp_size // 2, sp_size - 2
    planes = sp_size // 2
    chip, core = tp_size // 2, 1
    place = lax.axis_index("sp")
    on_side = (place & 1) == 1
    low = (place & 2) == 2
    high = (place & 4) == 4
    bf16, f32 = jnp.bfloat16, jnp.float32

    def swap(array, axis, distance):
        count = sp_size if axis == "sp" else tp_size
        return lax.ppermute(array, axis, [(i, i ^ distance) for i in range(count)])

    def swap_both(array, first, second):
        pairs = [
            (i * tp_size + j, (i ^ first) * tp_size + (j ^ second))
            for i in range(sp_size)
            for j in range(tp_size)
        ]
        return lax.ppermute(array, ("sp", "tp"), pairs)

    inner = [i for i in range(sp_size) if 0 < i // 2 < planes - 1]
    middle_pairs = [(i, i ^ far) for i in inner]
    outward_pairs = [(i, i ^ near) for i in inner]

    def three(first, second, third):
        third = swap(third, "sp", far)
        second = swap(second, "sp", across)
        return swap(first, "sp", near), second, third

    def along_line(weight):
        near_one = swap(weight, "sp", near)
        middle_one = lax.ppermute(weight, "sp", middle_pairs)
        middle_two = lax.ppermute(near_one, "sp", middle_pairs)
        outer_one = lax.ppermute(middle_one, "sp", outward_pairs)
        outer_two = lax.ppermute(middle_two, "sp", outward_pairs)
        return near_one, middle_one, outer_one, middle_two, outer_two

    def planes_by_distance(n):
        n = [jnp.where(low, n[k ^ 1], n[k]) for k in range(4)]
        return [jnp.where(high, n[k ^ 2], n[k]) for k in range(4)]

    def planes_along_line(n):
        first, second = jnp.where(low, n[1], n[0]), jnp.where(low, n[0], n[1])
        return [
            jnp.where(high, n[3], first),
            jnp.where(high, n[2], second),
            jnp.where(high, first, n[2]),
            jnp.where(high, second, n[3]),
        ]

    def side_by_side(same, other):
        return jnp.concatenate(
            [jnp.where(on_side, other, same), jnp.where(on_side, same, other)], axis=1
        )

    def plane_sum(ours, given_away):
        ours = ours + swap(given_away, "tp", core).astype(f32)
        half_rows = ours.shape[0] // 2
        from_chip = swap(ours[half_rows:].astype(bf16), "tp", chip)
        ours = ours[:half_rows] + from_chip.astype(f32)
        rows = half_rows // planes
        blocks = [ours[k * rows : (k + 1) * rows] for k in range(planes)]
        others = three(*(block.astype(bf16) for block in blocks[1:]))
        blocks = [blocks[0], *(block.astype(f32) for block in others)]
        middle = ours.shape[1] // 2
        blocks = [side_by_side(block[:, :middle], block[:, middle:]) for block in blocks]
        return jnp.concatenate(planes_by_distance(blocks), axis=1)

    def scatter_sum(ours, given_away, ordered):
        ours = ours + swap(given_away, "tp", core).astype(f32)
        rows = ours.shape[0] // 4
        rounded = ours.astype(bf16)
        from_both = swap_both(rounded[3 * rows :], side, chip)
        from_side = swap(rounded[2 * rows : 3 * rows], "sp", side)
        from_chip = swap(rounded[rows : 2 * rows], "tp", chip)
        same = ours[:rows] + from_chip.astype(f32)
        other = from_side.astype(f32) + from_both.astype(f32)
        piece = same.shape[1] // planes
        joined = []
        for k in range(planes):
            a, b = (array[:, k * piece : (k + 1) * piece] for array in (same, other))
            joined.append(side_by_side(a, b))
        return jnp.concatenate(ordered(joined), axis=1)

    tokens = query_first.shape[0]
    rows = tokens // tp_size
    head_lanes = 2 * query_first.shape[1] // planes
    value_size = head_gain.shape[0]

    streams = (query_first, key_first, query_second, key_second, values)
    dealt, extra = kernel(
        functools.partial(deal_body, sp_size=sp_size, tp_size=tp_size),
        (
            jax.ShapeDtypeStruct((planes, tokens, 2 * head_lanes + value_size), bf16),
            jax.ShapeDtypeStruct((2, value_size), f32),
        ),
        (),
        (*streams, head_gain.reshape(1, -1), lambda_weight),
        [pltpu.VMEM(array.shape, bf16) for array in streams]
        + [
            pltpu.VMEM((1, value_size), f32),
            pltpu.SMEM(lambda_weight.shape, f32),
            pltpu.SemaphoreType.DMA((7,)),
        ],
    )
    first, second, third = three(dealt[1], dealt[2], dealt[3])
    early = swap(jnp.concatenate([dealt[0][:, head_lanes:], first[:, head_lanes:]], 0), "sp", side)
    late = swap(jnp.concatenate([second[:, head_lanes:], third[:, head_lanes:]], 0), "sp", side)
    attended = kernel(
        attention_body,
        jax.ShapeDtypeStruct((planes, tokens, value_size), bf16),
        (extra, dealt[0], first, second, third, early, late),
        scratch=[
            pltpu.VMEM((2 * planes * tokens, head_lanes), bf16),
            pltpu.VMEM((2 * planes * tokens, value_size), bf16),
        ],
    )
    width = residual.shape[1]
    part = (planes * tokens // 2, width // planes)
    projected = kernel(
        functools.partial(project_body, tp_size=tp_size),
        (jax.ShapeDtypeStruct(part, f32), jax.ShapeDtypeStruct(part, bf16)),
        (attended, *three(attended, attended, attended), swap(out_weight, "sp", side)),
        (out_weight,),
        [
            pltpu.VMEM(out_weight.shape, bf16),
            pltpu.VMEM((planes * tokens, out_weight.shape[1]), bf16),
            pltpu.SemaphoreType.DMA,
        ],
    )
    summed = plane_sum(*projected)
    after_attention = (residual.astype(f32) + summed).astype(bf16)
    stream = after_attention.astype(f32)
    scaled_rows = stream * lax.rsqrt(jnp.mean(stream * stream, axis=-1, keepdims=True) + epsilon)
    normed = (scaled_rows * norm_gain).astype(bf16)

    from_both = swap_both(normed, side, chip)
    from_side = swap(normed, "sp", side)
    from_chip = swap(normed, "tp", chip)
    four = jnp.concatenate([normed, from_chip, from_side, from_both], axis=0)
    units = gate_weight.shape[1]
    tile = 256
    sizes = [min(tile, units - start) for start in range(0, units, tile) for _ in range(2)]
    hidden = kernel(
        functools.partial(gate_body, tile=tile),
        jax.ShapeDtypeStruct((8 * rows, units), bf16),
        (four, swap(four, "tp", core)),
        (gate_weight, up_weight),
        [pltpu.VMEM((8 * rows, residual.shape[1]), bf16)]
        + [pltpu.VMEM((residual.shape[1], size), bf16) for size in sizes]
        + [pltpu.SemaphoreType.DMA((len(sizes),))],
        limit=24,
    )
    half = (4 * rows, width // 2)
    halves = (jax.ShapeDtypeStruct(half, f32), jax.ShapeDtypeStruct(half, bf16))
    middle = down_weight.shape[0] // 2
    fed = kernel(
        functools.partial(down_body, sp_size=sp_size),
        halves,
        (hidden, down_weight, *along_line(down_weight[:middle]), *along_line(down_weight[middle:])),
    )
    return (stream + scatter_sum(*fed, planes_along_line)).astype(bf16)


def solution(mesh):
    sp_size, tp_size = mesh.shape["sp"], mesh.shape["tp"]

    def local(*arrays):
        total_tokens = arrays[1].shape[0] * sp_size
        short = total_tokens <= arrays[0].shape[1]
        if short and (sp_size, tp_size) == (8, 4):
            return moved_local(sp_size, tp_size, *arrays)
        return gathered_local(*arrays)

    return jax.shard_map(
        local,
        mesh=mesh,
        in_specs=(
            P(("sp", "tp"), None),
            P("sp", "tp"),
            P("sp", "tp"),
            P("sp", "tp"),
            P("sp", "tp"),
            P("sp", "tp"),
            P("tp"),
            P(),
            P("sp", "tp"),
            P(),
            P(None, "tp"),
            P(None, "tp"),
            P("sp", "tp"),
        ),
        out_specs=P(("sp", "tp"), None),
        check_vma=False,
    )
```

```python
import functools
import math

import jax
import jax.numpy as jnp
from jax import lax
from jax.experimental import pallas as pl
from jax.experimental.pallas import tpu as pltpu
from jax.sharding import PartitionSpec as P


epsilon = 1e-06


def map_update(state_in, queries, key_rows, value_block, score_scale):
    maxima, totals, accumulated = state_in
    scores = (
        jnp.einsum("thd,khd->htk", queries, key_rows, preferred_element_type=jnp.float32)
        * score_scale
    )
    newest = jnp.maximum(maxima, jnp.max(scores, axis=-1))
    factor = jnp.exp(maxima - newest)
    weights = jnp.exp(scores - newest[:, :, None])
    totals = totals * factor + jnp.sum(weights, axis=-1)
    product = jnp.einsum(
        "htk,khe->the",
        weights.astype(jnp.bfloat16),
        value_block,
        preferred_element_type=jnp.float32,
    )
    accumulated = accumulated * factor.T[:, :, None] + product
    return (newest, totals, accumulated)


def gathered_local(
    residual,
    query_first,
    key_first,
    query_second,
    key_second,
    values,
    lambda_weight,
    head_gain,
    out_weight,
    norm_gain,
    gate_weight,
    up_weight,
    down_weight,
):
    tokens_here = query_first.shape[0]
    head_count = lambda_weight.shape[0]
    head_size = query_first.shape[1] // head_count
    value_size = values.shape[1] // head_count
    score_scale = head_size ** (-0.5)
    queries_first = query_first.reshape(tokens_here, head_count, head_size)
    queries_second = query_second.reshape(tokens_here, head_count, head_size)
    empty_stats = (
        jnp.full((head_count, tokens_here), -jnp.inf, jnp.float32),
        jnp.zeros((head_count, tokens_here), jnp.float32),
        jnp.zeros((tokens_here, head_count, value_size), jnp.float32),
    )
    start_state = (empty_stats, empty_stats)
    keys_one = lax.all_gather(key_first, "sp", axis=0, tiled=True)
    row_count = keys_one.shape[0]
    block_rows = math.gcd(row_count, 1024)
    blocks = (
        keys_one.reshape(row_count // block_rows, block_rows, head_count, head_size),
        lax.all_gather(key_second, "sp", axis=0, tiled=True).reshape(
            row_count // block_rows, block_rows, head_count, head_size
        ),
        lax.all_gather(values, "sp", axis=0, tiled=True).reshape(
            row_count // block_rows, block_rows, head_count, value_size
        ),
    )

    def advance(current, block_keys):
        return (
            (
                map_update(current[0], queries_first, block_keys[0], block_keys[2], score_scale),
                map_update(current[1], queries_second, block_keys[1], block_keys[2], score_scale),
            ),
            None,
        )

    statistics = lax.scan(advance, start_state, blocks)[0]

    def finish(map_stats):
        return map_stats[2] / map_stats[1].T[:, :, None]

    difference = finish(statistics[0]) - lambda_weight[None, :, None] * finish(statistics[1])
    scaled = difference * lax.rsqrt(
        jnp.mean(difference * difference, axis=-1, keepdims=True) + epsilon
    )
    attended = (
        (scaled * head_gain).astype(jnp.bfloat16).reshape(tokens_here, head_count * value_size)
    )
    partial_value = lax.dot_general(
        attended,
        lax.all_gather(out_weight, "sp", axis=0, tiled=True),
        (((1,), (1,)), ((), ())),
        preferred_element_type=jnp.float32,
    )
    summed = lax.psum_scatter(
        partial_value.astype(jnp.bfloat16), "tp", scatter_dimension=0, tiled=True
    ).astype(jnp.float32)
    after_attention = (residual.astype(jnp.float32) + summed).astype(jnp.bfloat16)
    stream = after_attention.astype(jnp.float32)
    scaled_rows = stream * lax.rsqrt(jnp.mean(stream * stream, axis=-1, keepdims=True) + epsilon)
    shard_piece = lax.all_gather(
        (scaled_rows * norm_gain).astype(jnp.bfloat16), "tp", axis=0, tiled=True
    )
    gate_part = jnp.dot(shard_piece, gate_weight, preferred_element_type=jnp.float32)
    up_part = jnp.dot(shard_piece, up_weight, preferred_element_type=jnp.float32)
    hidden = (jax.nn.silu(gate_part) * up_part).astype(jnp.bfloat16)
    down_partial = lax.dot_general(
        hidden,
        lax.all_gather(down_weight, "sp", axis=0, tiled=True),
        (((1,), (1,)), ((), ())),
        preferred_element_type=jnp.float32,
    )
    feed_out = lax.psum_scatter(
        down_partial.astype(jnp.bfloat16), "tp", scatter_dimension=0, tiled=True
    ).astype(jnp.float32)
    return (after_attention.astype(jnp.float32) + feed_out).astype(jnp.bfloat16)


def deal_body(*refs, sp_size, tp_size):
    sources, out_ref, extra_ref, arrived, sems = refs[:7], refs[7], refs[8], refs[9:16], refs[16]
    copies = [
        pltpu.make_async_copy(source, to, sems.at[index])
        for index, (source, to) in enumerate(zip(sources, arrived))
    ]
    for copy in copies:
        copy.start()
    for copy in copies:
        copy.wait()
    qf_ref, kf_ref, qs_ref, ks_ref, v_ref, gain_ref, lambda_ref = arrived
    here = lax.axis_index("sp") // 2
    member = lax.axis_index("tp")
    heads = sp_size // 2
    rows = qf_ref.shape[0] // tp_size
    size = qf_ref.shape[1] // heads
    value_size = v_ref.shape[1] // heads
    extra_ref[0:1] = gain_ref[...]
    extra_ref[1:2] = jnp.full((1, value_size), lambda_ref[here], jnp.float32)
    for block in range(tp_size):
        at = pl.ds(pl.multiple_of((member ^ block) * rows, rows), rows)
        for head in range(heads):
            columns = slice(head * size, (head + 1) * size)
            narrow = [ref[at, columns] for ref in (qf_ref, qs_ref, kf_ref, ks_ref)]
            out_ref[here ^ head, block * rows : (block + 1) * rows, :] = jnp.concatenate(
                narrow + [v_ref[at, head * value_size : (head + 1) * value_size]], axis=1
            )


def attention_body(
    extra_ref, a_ref, b_ref, c_ref, d_ref, ab_ref, cd_ref, out_ref, k_ref, v_ref
):
    rows = a_ref.shape[0]
    gain, weight = extra_ref[0:1], extra_ref[1:2]
    lanes = a_ref.shape[1] - ab_ref.shape[1]
    head_size = lanes // 2
    scale = head_size ** (-0.5)
    exact = math.frexp(scale)[0] == 0.5
    queries = (a_ref, b_ref, c_ref, d_ref)
    for index, ref in enumerate(queries):
        k_ref[index * rows : (index + 1) * rows] = ref[:, lanes : 2 * lanes]
        v_ref[index * rows : (index + 1) * rows] = ref[:, 2 * lanes :]
    for index, ref in enumerate((ab_ref, cd_ref)):
        at = slice((4 + 2 * index) * rows, (6 + 2 * index) * rows)
        k_ref[at] = ref[:, :lanes]
        v_ref[at] = ref[:, lanes:]
    lane = lax.broadcasted_iota(jnp.int32, (rows, lanes), 1)

    def one_map(query, which):
        wanted = (lane < head_size) if which == 0 else (lane >= head_size)
        scores = lax.dot_general(
            jnp.where(wanted, query, jnp.zeros_like(query)),
            k_ref[...],
            (((1,), (1,)), ((), ())),
            preferred_element_type=jnp.float32,
        )
        if not exact:
            scores = scores * scale
        shifted = jnp.exp(scores - scores.max(axis=-1, keepdims=True))
        total = shifted.sum(axis=-1, keepdims=True)
        product = jnp.dot(
            shifted.astype(jnp.bfloat16), v_ref[...], preferred_element_type=jnp.float32
        )
        return product / total

    for index, ref in enumerate(queries):
        query = ref[:, :lanes]
        if exact:
            query = query * jnp.asarray(scale, query.dtype)
        difference = one_map(query, 0) - weight * one_map(query, 1)
        scaled = difference * lax.rsqrt(
            jnp.mean(difference * difference, axis=-1, keepdims=True) + epsilon
        )
        out_ref[index] = (scaled * gain).astype(out_ref.dtype)


def project_body(
    a_ref, b_ref, c_ref, d_ref, other_ref, source, kept_ref, sent_ref, own_ref, heads_ref, sem, *, tp_size
):
    copy = pltpu.make_async_copy(source, own_ref, sem)
    copy.start()
    here = lax.axis_index("sp") // 2
    planes, tokens, size = a_ref.shape
    for distance, ref in enumerate((a_ref, b_ref, c_ref, d_ref)):
        columns = pl.ds(pl.multiple_of((here ^ distance) * size, size), size)
        for block in range(planes):
            heads_ref[block * tokens : (block + 1) * tokens, columns] = ref[distance ^ block]
    rows = tokens // tp_size
    width = own_ref.shape[0]
    for index, ref in ((1, other_ref), (0, own_ref)):
        if index == 0:
            copy.wait()
        columns = slice(index * width, (index + 1) * width)
        product = lax.dot_general(
            heads_ref[...], ref[...], (((1,), (1,)), ((), ())), preferred_element_type=jnp.float32
        )
        for block in range(planes):
            for chip in range(tp_size // 2):
                to = slice((chip * planes + block) * rows, (chip * planes + block + 1) * rows)
                at = block * tokens + chip * 2 * rows
                kept_ref[to, columns] = product[at : at + rows]
                sent_ref[to, columns] = product[at + rows : at + 2 * rows].astype(sent_ref.dtype)


def gate_body(here_ref, there_ref, gate_ref, up_ref, hidden_ref, both_ref, *rest, tile):
    rows = here_ref.shape[0]
    units = gate_ref.shape[1]
    starts = range(0, units, tile)
    buffers, sems = rest[:-1], rest[-1]
    copies = []
    for index, start in enumerate(starts):
        columns = pl.ds(start, min(tile, units - start))
        pair = [
            pltpu.make_async_copy(
                ref.at[:, columns], buffers[2 * index + which], sems.at[2 * index + which]
            )
            for which, ref in enumerate((gate_ref, up_ref))
        ]
        for copy in pair:
            copy.start()
        copies.append(pair)
    both_ref[:rows] = here_ref[...]
    both_ref[rows:] = there_ref[...]
    for index, start in enumerate(starts):
        for copy in copies[index]:
            copy.wait()
        gate, up = (
            jnp.dot(
                both_ref[...], buffers[2 * index + which][...], preferred_element_type=jnp.float32
            )
            for which in range(2)
        )
        hidden = gate / (1.0 + jnp.exp(-gate)) * up
        hidden_ref[:, start : start + gate.shape[1]] = hidden.astype(hidden_ref.dtype)


def down_body(hidden_ref, own_ref, *refs, sp_size):
    parts, (kept_ref, sent_ref) = refs[:-2], refs[-2:]
    parts = [parts[start : start + 5] for start in range(0, len(parts), 5)]
    place = lax.axis_index("sp") // 2
    inner = (place > 0) & (place < sp_size // 2 - 1)
    rows = kept_ref.shape[0]
    width = own_ref.shape[0]

    def third(part):
        return jnp.where(inner, part[1][...], part[2][...])

    def last(part):
        return jnp.where(inner, part[3][...], part[4][...])

    pieces = (
        lambda: own_ref[...],
        lambda: jnp.concatenate([part[0][...] for part in parts], axis=0),
        lambda: jnp.concatenate([third(part) for part in parts], axis=0),
        lambda: jnp.concatenate([last(part) for part in parts], axis=0),
    )
    for index, piece in enumerate(pieces):
        product = lax.dot_general(
            hidden_ref[...], piece(), (((1,), (1,)), ((), ())), preferred_element_type=jnp.float32
        )
        columns = slice(index * width, (index + 1) * width)
        kept_ref[:, columns] = product[:rows]
        sent_ref[:, columns] = product[rows:].astype(sent_ref.dtype)


def kernel(body, out_shape, near, away=(), scratch=(), limit=16):
    vmem = pl.BlockSpec(memory_space=pltpu.VMEM)
    many = isinstance(out_shape, tuple)
    call = pl.pallas_call(
        body,
        out_shape=out_shape,
        in_specs=[vmem] * len(near) + [pl.BlockSpec(memory_space=pltpu.HBM)] * len(away),
        out_specs=(vmem,) * len(out_shape) if many else vmem,
        scratch_shapes=list(scratch),
        compiler_params=pltpu.CompilerParams(vmem_limit_bytes=limit * 2**20),
    )
    return call(*near, *(pltpu.with_memory_space_constraint(array, pltpu.HBM) for array in away))


def moved_local(
    sp_size,
    tp_size,
    residual,
    query_first,
    key_first,
    query_second,
    key_second,
    values,
    lambda_weight,
    head_gain,
    out_weight,
    norm_gain,
    gate_weight,
    up_weight,
    down_weight,
):
    side, near, across, far = 1, 2, sp_size // 2, sp_size - 2
    planes = sp_size // 2
    chip, core = tp_size // 2, 1
    place = lax.axis_index("sp")
    on_side = (place & 1) == 1
    low = (place & 2) == 2
    high = (place & 4) == 4
    bf16, f32 = jnp.bfloat16, jnp.float32

    def swap(array, axis, distance):
        count = sp_size if axis == "sp" else tp_size
        return lax.ppermute(array, axis, [(i, i ^ distance) for i in range(count)])

    def swap_both(array, first, second):
        pairs = [
            (i * tp_size + j, (i ^ first) * tp_size + (j ^ second))
            for i in range(sp_size)
            for j in range(tp_size)
        ]
        return lax.ppermute(array, ("sp", "tp"), pairs)

    inner = [i for i in range(sp_size) if 0 < i // 2 < planes - 1]
    middle_pairs = [(i, i ^ far) for i in inner]
    outward_pairs = [(i, i ^ near) for i in inner]

    def three(first, second, third):
        third = swap(third, "sp", far)
        second = swap(second, "sp", across)
        return swap(first, "sp", near), second, third

    def along_line(weight):
        near_one = swap(weight, "sp", near)
        middle_one = lax.ppermute(weight, "sp", middle_pairs)
        middle_two = lax.ppermute(near_one, "sp", middle_pairs)
        outer_one = lax.ppermute(middle_one, "sp", outward_pairs)
        outer_two = lax.ppermute(middle_two, "sp", outward_pairs)
        return near_one, middle_one, outer_one, middle_two, outer_two

    def planes_by_distance(n):
        n = [jnp.where(low, n[k ^ 1], n[k]) for k in range(4)]
        return [jnp.where(high, n[k ^ 2], n[k]) for k in range(4)]

    def planes_along_line(n):
        first, second = jnp.where(low, n[1], n[0]), jnp.where(low, n[0], n[1])
        return [
            jnp.where(high, n[3], first),
            jnp.where(high, n[2], second),
            jnp.where(high, first, n[2]),
            jnp.where(high, second, n[3]),
        ]

    def side_by_side(same, other):
        return jnp.concatenate(
            [jnp.where(on_side, other, same), jnp.where(on_side, same, other)], axis=1
        )

    def plane_sum(ours, given_away):
        ours = ours + swap(given_away, "tp", core).astype(f32)
        half_rows = ours.shape[0] // 2
        from_chip = swap(ours[half_rows:].astype(bf16), "tp", chip)
        ours = ours[:half_rows] + from_chip.astype(f32)
        rows = half_rows // planes
        blocks = [ours[k * rows : (k + 1) * rows] for k in range(planes)]
        others = three(*(block.astype(bf16) for block in blocks[1:]))
        blocks = [blocks[0], *(block.astype(f32) for block in others)]
        middle = ours.shape[1] // 2
        blocks = [side_by_side(block[:, :middle], block[:, middle:]) for block in blocks]
        return jnp.concatenate(planes_by_distance(blocks), axis=1)

    def scatter_sum(ours, given_away, ordered):
        ours = ours + swap(given_away, "tp", core).astype(f32)
        rows = ours.shape[0] // 4
        rounded = ours.astype(bf16)
        from_both = swap_both(rounded[3 * rows :], side, chip)
        from_side = swap(rounded[2 * rows : 3 * rows], "sp", side)
        from_chip = swap(rounded[rows : 2 * rows], "tp", chip)
        same = ours[:rows] + from_chip.astype(f32)
        other = from_side.astype(f32) + from_both.astype(f32)
        piece = same.shape[1] // planes
        joined = []
        for k in range(planes):
            a, b = (array[:, k * piece : (k + 1) * piece] for array in (same, other))
            joined.append(side_by_side(a, b))
        return jnp.concatenate(ordered(joined), axis=1)

    tokens = query_first.shape[0]
    rows = tokens // tp_size
    head_lanes = 2 * query_first.shape[1] // planes
    value_size = head_gain.shape[0]

    streams = (query_first, key_first, query_second, key_second, values)
    dealt, extra = kernel(
        functools.partial(deal_body, sp_size=sp_size, tp_size=tp_size),
        (
            jax.ShapeDtypeStruct((planes, tokens, 2 * head_lanes + value_size), bf16),
            jax.ShapeDtypeStruct((2, value_size), f32),
        ),
        (),
        (*streams, head_gain.reshape(1, -1), lambda_weight),
        [pltpu.VMEM(array.shape, bf16) for array in streams]
        + [
            pltpu.VMEM((1, value_size), f32),
            pltpu.SMEM(lambda_weight.shape, f32),
            pltpu.SemaphoreType.DMA((7,)),
        ],
    )
    first, second, third = three(dealt[1], dealt[2], dealt[3])
    early = swap(jnp.concatenate([dealt[0][:, head_lanes:], first[:, head_lanes:]], 0), "sp", side)
    late = swap(jnp.concatenate([second[:, head_lanes:], third[:, head_lanes:]], 0), "sp", side)
    attended = kernel(
        attention_body,
        jax.ShapeDtypeStruct((planes, tokens, value_size), bf16),
        (extra, dealt[0], first, second, third, early, late),
        scratch=[
            pltpu.VMEM((2 * planes * tokens, head_lanes), bf16),
            pltpu.VMEM((2 * planes * tokens, value_size), bf16),
        ],
    )
    width = residual.shape[1]
    part = (planes * tokens // 2, width // planes)
    projected = kernel(
        functools.partial(project_body, tp_size=tp_size),
        (jax.ShapeDtypeStruct(part, f32), jax.ShapeDtypeStruct(part, bf16)),
        (attended, *three(attended, attended, attended), swap(out_weight, "sp", side)),
        (out_weight,),
        [
            pltpu.VMEM(out_weight.shape, bf16),
            pltpu.VMEM((planes * tokens, out_weight.shape[1]), bf16),
            pltpu.SemaphoreType.DMA,
        ],
    )
    summed = plane_sum(*projected)
    after_attention = (residual.astype(f32) + summed).astype(bf16)
    stream = after_attention.astype(f32)
    scaled_rows = stream * lax.rsqrt(jnp.mean(stream * stream, axis=-1, keepdims=True) + epsilon)
    normed = (scaled_rows * norm_gain).astype(bf16)

    from_both = swap_both(normed, side, chip)
    from_side = swap(normed, "sp", side)
    from_chip = swap(normed, "tp", chip)
    four = jnp.concatenate([normed, from_chip, from_side, from_both], axis=0)
    units = gate_weight.shape[1]
    tile = 256
    sizes = [min(tile, units - start) for start in range(0, units, tile) for _ in range(2)]
    hidden = kernel(
        functools.partial(gate_body, tile=tile),
        jax.ShapeDtypeStruct((8 * rows, units), bf16),
        (four, swap(four, "tp", core)),
        (gate_weight, up_weight),
        [pltpu.VMEM((8 * rows, residual.shape[1]), bf16)]
        + [pltpu.VMEM((residual.shape[1], size), bf16) for size in sizes]
        + [pltpu.SemaphoreType.DMA((len(sizes),))],
        limit=24,
    )
    half = (4 * rows, width // 2)
    halves = (jax.ShapeDtypeStruct(half, f32), jax.ShapeDtypeStruct(half, bf16))
    middle = down_weight.shape[0] * 5 // 8
    fed = kernel(
        functools.partial(down_body, sp_size=sp_size),
        halves,
        (hidden, down_weight, *along_line(down_weight[:middle]), *along_line(down_weight[middle:])),
    )
    return (stream + scatter_sum(*fed, planes_along_line)).astype(bf16)


def solution(mesh):
    sp_size, tp_size = mesh.shape["sp"], mesh.shape["tp"]

    def local(*arrays):
        total_tokens = arrays[1].shape[0] * sp_size
        short = total_tokens <= arrays[0].shape[1]
        if short and (sp_size, tp_size) == (8, 4):
            return moved_local(sp_size, tp_size, *arrays)
        return gathered_local(*arrays)

    return jax.shard_map(
        local,
        mesh=mesh,
        in_specs=(
            P(("sp", "tp"), None),
            P("sp", "tp"),
            P("sp", "tp"),
            P("sp", "tp"),
            P("sp", "tp"),
            P("sp", "tp"),
            P("tp"),
            P(),
            P("sp", "tp"),
            P(),
            P(None, "tp"),
            P(None, "tp"),
            P("sp", "tp"),
        ),
        out_specs=P(("sp", "tp"), None),
        check_vma=False,
    )
```

```python
import functools
import math

import jax
import jax.numpy as jnp
from jax import lax
from jax.experimental import pallas as pl
from jax.experimental.pallas import tpu as pltpu
from jax.sharding import PartitionSpec as P


epsilon = 1e-06


def map_update(state_in, queries, key_rows, value_block, score_scale):
    maxima, totals, accumulated = state_in
    scores = (
        jnp.einsum("thd,khd->htk", queries, key_rows, preferred_element_type=jnp.float32)
        * score_scale
    )
    newest = jnp.maximum(maxima, jnp.max(scores, axis=-1))
    factor = jnp.exp(maxima - newest)
    weights = jnp.exp(scores - newest[:, :, None])
    totals = totals * factor + jnp.sum(weights, axis=-1)
    product = jnp.einsum(
        "htk,khe->the",
        weights.astype(jnp.bfloat16),
        value_block,
        preferred_element_type=jnp.float32,
    )
    accumulated = accumulated * factor.T[:, :, None] + product
    return (newest, totals, accumulated)


def gathered_local(
    residual,
    query_first,
    key_first,
    query_second,
    key_second,
    values,
    lambda_weight,
    head_gain,
    out_weight,
    norm_gain,
    gate_weight,
    up_weight,
    down_weight,
):
    tokens_here = query_first.shape[0]
    head_count = lambda_weight.shape[0]
    head_size = query_first.shape[1] // head_count
    value_size = values.shape[1] // head_count
    score_scale = head_size ** (-0.5)
    queries_first = query_first.reshape(tokens_here, head_count, head_size)
    queries_second = query_second.reshape(tokens_here, head_count, head_size)
    empty_stats = (
        jnp.full((head_count, tokens_here), -jnp.inf, jnp.float32),
        jnp.zeros((head_count, tokens_here), jnp.float32),
        jnp.zeros((tokens_here, head_count, value_size), jnp.float32),
    )
    start_state = (empty_stats, empty_stats)
    keys_one = lax.all_gather(key_first, "sp", axis=0, tiled=True)
    row_count = keys_one.shape[0]
    block_rows = math.gcd(row_count, 1024)
    blocks = (
        keys_one.reshape(row_count // block_rows, block_rows, head_count, head_size),
        lax.all_gather(key_second, "sp", axis=0, tiled=True).reshape(
            row_count // block_rows, block_rows, head_count, head_size
        ),
        lax.all_gather(values, "sp", axis=0, tiled=True).reshape(
            row_count // block_rows, block_rows, head_count, value_size
        ),
    )

    def advance(current, block_keys):
        return (
            (
                map_update(current[0], queries_first, block_keys[0], block_keys[2], score_scale),
                map_update(current[1], queries_second, block_keys[1], block_keys[2], score_scale),
            ),
            None,
        )

    statistics = lax.scan(advance, start_state, blocks)[0]

    def finish(map_stats):
        return map_stats[2] / map_stats[1].T[:, :, None]

    difference = finish(statistics[0]) - lambda_weight[None, :, None] * finish(statistics[1])
    scaled = difference * lax.rsqrt(
        jnp.mean(difference * difference, axis=-1, keepdims=True) + epsilon
    )
    attended = (
        (scaled * head_gain).astype(jnp.bfloat16).reshape(tokens_here, head_count * value_size)
    )
    partial_value = lax.dot_general(
        attended,
        lax.all_gather(out_weight, "sp", axis=0, tiled=True),
        (((1,), (1,)), ((), ())),
        preferred_element_type=jnp.float32,
    )
    summed = lax.psum_scatter(
        partial_value.astype(jnp.bfloat16), "tp", scatter_dimension=0, tiled=True
    ).astype(jnp.float32)
    after_attention = (residual.astype(jnp.float32) + summed).astype(jnp.bfloat16)
    stream = after_attention.astype(jnp.float32)
    scaled_rows = stream * lax.rsqrt(jnp.mean(stream * stream, axis=-1, keepdims=True) + epsilon)
    shard_piece = lax.all_gather(
        (scaled_rows * norm_gain).astype(jnp.bfloat16), "tp", axis=0, tiled=True
    )
    gate_part = jnp.dot(shard_piece, gate_weight, preferred_element_type=jnp.float32)
    up_part = jnp.dot(shard_piece, up_weight, preferred_element_type=jnp.float32)
    hidden = (jax.nn.silu(gate_part) * up_part).astype(jnp.bfloat16)
    down_partial = lax.dot_general(
        hidden,
        lax.all_gather(down_weight, "sp", axis=0, tiled=True),
        (((1,), (1,)), ((), ())),
        preferred_element_type=jnp.float32,
    )
    feed_out = lax.psum_scatter(
        down_partial.astype(jnp.bfloat16), "tp", scatter_dimension=0, tiled=True
    ).astype(jnp.float32)
    return (after_attention.astype(jnp.float32) + feed_out).astype(jnp.bfloat16)


def deal_body(*refs, sp_size, tp_size):
    sources, out_ref, extra_ref, arrived, sems = refs[:7], refs[7], refs[8], refs[9:16], refs[16]
    copies = [
        pltpu.make_async_copy(source, to, sems.at[index])
        for index, (source, to) in enumerate(zip(sources, arrived))
    ]
    for copy in copies:
        copy.start()
    for copy in copies:
        copy.wait()
    qf_ref, kf_ref, qs_ref, ks_ref, v_ref, gain_ref, lambda_ref = arrived
    here = lax.axis_index("sp") // 2
    member = lax.axis_index("tp")
    heads = sp_size // 2
    rows = qf_ref.shape[0] // tp_size
    size = qf_ref.shape[1] // heads
    value_size = v_ref.shape[1] // heads
    extra_ref[0:1] = gain_ref[...]
    extra_ref[1:2] = jnp.full((1, value_size), lambda_ref[here], jnp.float32)
    for block in range(tp_size):
        at = pl.ds(pl.multiple_of((member ^ block) * rows, rows), rows)
        for head in range(heads):
            columns = slice(head * size, (head + 1) * size)
            narrow = [ref[at, columns] for ref in (qf_ref, qs_ref, kf_ref, ks_ref)]
            out_ref[here ^ head, block * rows : (block + 1) * rows, :] = jnp.concatenate(
                narrow + [v_ref[at, head * value_size : (head + 1) * value_size]], axis=1
            )


def attention_body(
    extra_ref, a_ref, b_ref, c_ref, d_ref, ab_ref, cd_ref, out_ref, k_ref, v_ref
):
    rows = a_ref.shape[0]
    gain, weight = extra_ref[0:1], extra_ref[1:2]
    lanes = a_ref.shape[1] - ab_ref.shape[1]
    head_size = lanes // 2
    scale = head_size ** (-0.5)
    exact = math.frexp(scale)[0] == 0.5
    queries = (a_ref, b_ref, c_ref, d_ref)
    for index, ref in enumerate(queries):
        k_ref[index * rows : (index + 1) * rows] = ref[:, lanes : 2 * lanes]
        v_ref[index * rows : (index + 1) * rows] = ref[:, 2 * lanes :]
    for index, ref in enumerate((ab_ref, cd_ref)):
        at = slice((4 + 2 * index) * rows, (6 + 2 * index) * rows)
        k_ref[at] = ref[:, :lanes]
        v_ref[at] = ref[:, lanes:]
    lane = lax.broadcasted_iota(jnp.int32, (rows, lanes), 1)

    def one_map(query, which):
        wanted = (lane < head_size) if which == 0 else (lane >= head_size)
        scores = lax.dot_general(
            jnp.where(wanted, query, jnp.zeros_like(query)),
            k_ref[...],
            (((1,), (1,)), ((), ())),
            preferred_element_type=jnp.float32,
        )
        if not exact:
            scores = scores * scale
        shifted = jnp.exp(scores - scores.max(axis=-1, keepdims=True))
        total = shifted.sum(axis=-1, keepdims=True)
        product = jnp.dot(
            shifted.astype(jnp.bfloat16), v_ref[...], preferred_element_type=jnp.float32
        )
        return product / total

    for index, ref in enumerate(queries):
        query = ref[:, :lanes]
        if exact:
            query = query * jnp.asarray(scale, query.dtype)
        difference = one_map(query, 0) - weight * one_map(query, 1)
        scaled = difference * lax.rsqrt(
            jnp.mean(difference * difference, axis=-1, keepdims=True) + epsilon
        )
        out_ref[index] = (scaled * gain).astype(out_ref.dtype)


def project_body(
    a_ref, b_ref, c_ref, d_ref, other_ref, source, kept_ref, sent_ref, own_ref, heads_ref, sem, *, tp_size
):
    copy = pltpu.make_async_copy(source, own_ref, sem)
    copy.start()
    here = lax.axis_index("sp") // 2
    planes, tokens, size = a_ref.shape
    for distance, ref in enumerate((a_ref, b_ref, c_ref, d_ref)):
        columns = pl.ds(pl.multiple_of((here ^ distance) * size, size), size)
        for block in range(planes):
            heads_ref[block * tokens : (block + 1) * tokens, columns] = ref[distance ^ block]
    rows = tokens // tp_size
    width = own_ref.shape[0]
    for index, ref in ((1, other_ref), (0, own_ref)):
        if index == 0:
            copy.wait()
        columns = slice(index * width, (index + 1) * width)
        product = lax.dot_general(
            heads_ref[...], ref[...], (((1,), (1,)), ((), ())), preferred_element_type=jnp.float32
        )
        for block in range(planes):
            for chip in range(tp_size // 2):
                to = slice((chip * planes + block) * rows, (chip * planes + block + 1) * rows)
                at = block * tokens + chip * 2 * rows
                kept_ref[to, columns] = product[at : at + rows]
                sent_ref[to, columns] = product[at + rows : at + 2 * rows].astype(sent_ref.dtype)


def gate_body(here_ref, there_ref, gate_ref, up_ref, hidden_ref, both_ref, *rest, tile):
    rows = here_ref.shape[0]
    units = gate_ref.shape[1]
    starts = range(0, units, tile)
    buffers, sems = rest[:-1], rest[-1]
    copies = []
    for index, start in enumerate(starts):
        columns = pl.ds(start, min(tile, units - start))
        pair = [
            pltpu.make_async_copy(
                ref.at[:, columns], buffers[2 * index + which], sems.at[2 * index + which]
            )
            for which, ref in enumerate((gate_ref, up_ref))
        ]
        for copy in pair:
            copy.start()
        copies.append(pair)
    both_ref[:rows] = here_ref[...]
    both_ref[rows:] = there_ref[...]
    for index, start in enumerate(starts):
        for copy in copies[index]:
            copy.wait()
        gate, up = (
            jnp.dot(
                both_ref[...], buffers[2 * index + which][...], preferred_element_type=jnp.float32
            )
            for which in range(2)
        )
        hidden = gate / (1.0 + jnp.exp(-gate)) * up
        hidden_ref[:, start : start + gate.shape[1]] = hidden.astype(hidden_ref.dtype)


def down_body(hidden_ref, *refs, pieces, sp_size):
    kept_ref, sent_ref = refs[-2:]
    refs = list(refs[:-2])
    place = lax.axis_index("sp") // 2
    inner = (place > 0) & (place < sp_size // 2 - 1)
    rows = kept_ref.shape[0]
    start = 0
    for parts, choices in pieces:
        values = []
        for _ in range(parts):
            part = [refs.pop(0)[...] for _ in range(choices)]
            values.append(part[0] if choices == 1 else jnp.where(inner, *part))
        piece = values[0] if parts == 1 else jnp.concatenate(values, axis=0)
        product = lax.dot_general(
            hidden_ref[...], piece, (((1,), (1,)), ((), ())), preferred_element_type=jnp.float32
        )
        columns = slice(start, start + piece.shape[0])
        kept_ref[:, columns] = product[:rows]
        sent_ref[:, columns] = product[rows:].astype(sent_ref.dtype)
        start += piece.shape[0]


def kernel(body, out_shape, near, away=(), scratch=(), limit=16):
    vmem = pl.BlockSpec(memory_space=pltpu.VMEM)
    many = isinstance(out_shape, tuple)
    call = pl.pallas_call(
        body,
        out_shape=out_shape,
        in_specs=[vmem] * len(near) + [pl.BlockSpec(memory_space=pltpu.HBM)] * len(away),
        out_specs=(vmem,) * len(out_shape) if many else vmem,
        scratch_shapes=list(scratch),
        compiler_params=pltpu.CompilerParams(vmem_limit_bytes=limit * 2**20),
    )
    return call(*near, *(pltpu.with_memory_space_constraint(array, pltpu.HBM) for array in away))


def moved_local(
    sp_size,
    tp_size,
    residual,
    query_first,
    key_first,
    query_second,
    key_second,
    values,
    lambda_weight,
    head_gain,
    out_weight,
    norm_gain,
    gate_weight,
    up_weight,
    down_weight,
):
    side, near, across, far = 1, 2, sp_size // 2, sp_size - 2
    planes = sp_size // 2
    chip, core = tp_size // 2, 1
    place = lax.axis_index("sp")
    on_side = (place & 1) == 1
    low = (place & 2) == 2
    high = (place & 4) == 4
    bf16, f32 = jnp.bfloat16, jnp.float32

    def swap(array, axis, distance):
        count = sp_size if axis == "sp" else tp_size
        return lax.ppermute(array, axis, [(i, i ^ distance) for i in range(count)])

    def swap_both(array, first, second):
        pairs = [
            (i * tp_size + j, (i ^ first) * tp_size + (j ^ second))
            for i in range(sp_size)
            for j in range(tp_size)
        ]
        return lax.ppermute(array, ("sp", "tp"), pairs)

    inner = [i for i in range(sp_size) if 0 < i // 2 < planes - 1]
    middle_pairs = [(i, i ^ far) for i in inner]
    outward_pairs = [(i, i ^ near) for i in inner]

    def three(first, second, third):
        third = swap(third, "sp", far)
        second = swap(second, "sp", across)
        return swap(first, "sp", near), second, third

    def along_line(weight):
        near_one = swap(weight, "sp", near)
        middle_one = lax.ppermute(weight, "sp", middle_pairs)
        middle_two = lax.ppermute(near_one, "sp", middle_pairs)
        outer_one = lax.ppermute(middle_one, "sp", outward_pairs)
        outer_two = lax.ppermute(middle_two, "sp", outward_pairs)
        return near_one, middle_one, outer_one, middle_two, outer_two

    def planes_by_distance(n):
        n = [jnp.where(low, n[k ^ 1], n[k]) for k in range(4)]
        return [jnp.where(high, n[k ^ 2], n[k]) for k in range(4)]

    def planes_along_line(n):
        first, second = jnp.where(low, n[1], n[0]), jnp.where(low, n[0], n[1])
        return [
            jnp.where(high, n[3], first),
            jnp.where(high, n[2], second),
            jnp.where(high, first, n[2]),
            jnp.where(high, second, n[3]),
        ]

    def side_by_side(same, other):
        return jnp.concatenate(
            [jnp.where(on_side, other, same), jnp.where(on_side, same, other)], axis=1
        )

    def plane_sum(ours, given_away):
        ours = ours + swap(given_away, "tp", core).astype(f32)
        half_rows = ours.shape[0] // 2
        from_chip = swap(ours[half_rows:].astype(bf16), "tp", chip)
        ours = ours[:half_rows] + from_chip.astype(f32)
        rows = half_rows // planes
        blocks = [ours[k * rows : (k + 1) * rows] for k in range(planes)]
        others = three(*(block.astype(bf16) for block in blocks[1:]))
        blocks = [blocks[0], *(block.astype(f32) for block in others)]
        middle = ours.shape[1] // 2
        blocks = [side_by_side(block[:, :middle], block[:, middle:]) for block in blocks]
        return jnp.concatenate(planes_by_distance(blocks), axis=1)

    def side_parts(ours, given_away):
        ours = ours + swap(given_away, "tp", core).astype(f32)
        rows = ours.shape[0] // 4
        rounded = ours.astype(bf16)
        from_both = swap_both(rounded[3 * rows :], side, chip)
        from_side = swap(rounded[2 * rows : 3 * rows], "sp", side)
        from_chip = swap(rounded[rows : 2 * rows], "tp", chip)
        return ours[:rows], from_chip, from_side, from_both

    def side_sum(own, from_chip, from_side, from_both):
        return own + from_chip.astype(f32), from_side.astype(f32) + from_both.astype(f32)

    tokens = query_first.shape[0]
    rows = tokens // tp_size
    head_lanes = 2 * query_first.shape[1] // planes
    value_size = head_gain.shape[0]

    streams = (query_first, key_first, query_second, key_second, values)
    dealt, extra = kernel(
        functools.partial(deal_body, sp_size=sp_size, tp_size=tp_size),
        (
            jax.ShapeDtypeStruct((planes, tokens, 2 * head_lanes + value_size), bf16),
            jax.ShapeDtypeStruct((2, value_size), f32),
        ),
        (),
        (*streams, head_gain.reshape(1, -1), lambda_weight),
        [pltpu.VMEM(array.shape, bf16) for array in streams]
        + [
            pltpu.VMEM((1, value_size), f32),
            pltpu.SMEM(lambda_weight.shape, f32),
            pltpu.SemaphoreType.DMA((7,)),
        ],
    )
    first, second, third = three(dealt[1], dealt[2], dealt[3])
    early = swap(jnp.concatenate([dealt[0][:, head_lanes:], first[:, head_lanes:]], 0), "sp", side)
    late = swap(jnp.concatenate([second[:, head_lanes:], third[:, head_lanes:]], 0), "sp", side)
    attended = kernel(
        attention_body,
        jax.ShapeDtypeStruct((planes, tokens, value_size), bf16),
        (extra, dealt[0], first, second, third, early, late),
        scratch=[
            pltpu.VMEM((2 * planes * tokens, head_lanes), bf16),
            pltpu.VMEM((2 * planes * tokens, value_size), bf16),
        ],
    )
    width = residual.shape[1]
    part = (planes * tokens // 2, width // planes)
    projected = kernel(
        functools.partial(project_body, tp_size=tp_size),
        (jax.ShapeDtypeStruct(part, f32), jax.ShapeDtypeStruct(part, bf16)),
        (attended, *three(attended, attended, attended), swap(out_weight, "sp", side)),
        (out_weight,),
        [
            pltpu.VMEM(out_weight.shape, bf16),
            pltpu.VMEM((planes * tokens, out_weight.shape[1]), bf16),
            pltpu.SemaphoreType.DMA,
        ],
    )
    summed = plane_sum(*projected)
    after_attention = (residual.astype(f32) + summed).astype(bf16)
    stream = after_attention.astype(f32)
    scaled_rows = stream * lax.rsqrt(jnp.mean(stream * stream, axis=-1, keepdims=True) + epsilon)
    normed = (scaled_rows * norm_gain).astype(bf16)

    from_both = swap_both(normed, side, chip)
    from_side = swap(normed, "sp", side)
    from_chip = swap(normed, "tp", chip)
    four = jnp.concatenate([normed, from_chip, from_side, from_both], axis=0)
    units = gate_weight.shape[1]
    tile = 256
    sizes = [min(tile, units - start) for start in range(0, units, tile) for _ in range(2)]
    hidden = kernel(
        functools.partial(gate_body, tile=tile),
        jax.ShapeDtypeStruct((8 * rows, units), bf16),
        (four, swap(four, "tp", core)),
        (gate_weight, up_weight),
        [pltpu.VMEM((8 * rows, residual.shape[1]), bf16)]
        + [pltpu.VMEM((residual.shape[1], size), bf16) for size in sizes]
        + [pltpu.SemaphoreType.DMA((len(sizes),))],
        limit=24,
    )
    middle = down_weight.shape[0] * 5 // 8
    ways = [along_line(down_weight[:middle]), along_line(down_weight[middle:])]

    def project_down(pieces, operands, columns):
        shape = (4 * rows, columns)
        parts = kernel(
            functools.partial(down_body, pieces=pieces, sp_size=sp_size),
            (jax.ShapeDtypeStruct(shape, f32), jax.ShapeDtypeStruct(shape, bf16)),
            (hidden, *operands),
        )
        return side_parts(*parts)

    piece = down_weight.shape[0]
    early_refs = [down_weight, *(way[0] for way in ways)]
    early_refs += [ref for way in ways for ref in way[1:3]]
    first = project_down(((1, 1), (2, 1), (2, 2)), early_refs, 3 * piece)
    last = project_down(((2, 2),), [ref for way in ways for ref in way[3:5]], piece)
    first, last = lax.optimization_barrier((first, last))
    first, last = side_sum(*first), side_sum(*last)
    joined = [
        side_by_side(*(array[:, k * piece : (k + 1) * piece] for array in first)) for k in range(3)
    ]
    joined.append(side_by_side(*last))
    fed = jnp.concatenate(planes_along_line(joined), axis=1)
    return (stream + fed).astype(bf16)


def solution(mesh):
    sp_size, tp_size = mesh.shape["sp"], mesh.shape["tp"]

    def local(*arrays):
        total_tokens = arrays[1].shape[0] * sp_size
        short = total_tokens <= arrays[0].shape[1]
        if short and (sp_size, tp_size) == (8, 4):
            return moved_local(sp_size, tp_size, *arrays)
        return gathered_local(*arrays)

    return jax.shard_map(
        local,
        mesh=mesh,
        in_specs=(
            P(("sp", "tp"), None),
            P("sp", "tp"),
            P("sp", "tp"),
            P("sp", "tp"),
            P("sp", "tp"),
            P("sp", "tp"),
            P("tp"),
            P(),
            P("sp", "tp"),
            P(),
            P(None, "tp"),
            P(None, "tp"),
            P("sp", "tp"),
        ),
        out_specs=P(("sp", "tp"), None),
        check_vma=False,
    )
```

```python
import functools
import math

import jax
import jax.numpy as jnp
from jax import lax
from jax.experimental import pallas as pl
from jax.experimental.pallas import tpu as pltpu
from jax.sharding import PartitionSpec as P


epsilon = 1e-06


def map_update(state_in, queries, key_rows, value_block, score_scale):
    maxima, totals, accumulated = state_in
    scores = (
        jnp.einsum("thd,khd->htk", queries, key_rows, preferred_element_type=jnp.float32)
        * score_scale
    )
    newest = jnp.maximum(maxima, jnp.max(scores, axis=-1))
    factor = jnp.exp(maxima - newest)
    weights = jnp.exp(scores - newest[:, :, None])
    totals = totals * factor + jnp.sum(weights, axis=-1)
    product = jnp.einsum(
        "htk,khe->the",
        weights.astype(jnp.bfloat16),
        value_block,
        preferred_element_type=jnp.float32,
    )
    accumulated = accumulated * factor.T[:, :, None] + product
    return (newest, totals, accumulated)


def gathered_local(
    residual,
    query_first,
    key_first,
    query_second,
    key_second,
    values,
    lambda_weight,
    head_gain,
    out_weight,
    norm_gain,
    gate_weight,
    up_weight,
    down_weight,
):
    tokens_here = query_first.shape[0]
    head_count = lambda_weight.shape[0]
    head_size = query_first.shape[1] // head_count
    value_size = values.shape[1] // head_count
    score_scale = head_size ** (-0.5)
    queries_first = query_first.reshape(tokens_here, head_count, head_size)
    queries_second = query_second.reshape(tokens_here, head_count, head_size)
    empty_stats = (
        jnp.full((head_count, tokens_here), -jnp.inf, jnp.float32),
        jnp.zeros((head_count, tokens_here), jnp.float32),
        jnp.zeros((tokens_here, head_count, value_size), jnp.float32),
    )
    start_state = (empty_stats, empty_stats)
    keys_one = lax.all_gather(key_first, "sp", axis=0, tiled=True)
    row_count = keys_one.shape[0]
    block_rows = math.gcd(row_count, 1024)
    blocks = (
        keys_one.reshape(row_count // block_rows, block_rows, head_count, head_size),
        lax.all_gather(key_second, "sp", axis=0, tiled=True).reshape(
            row_count // block_rows, block_rows, head_count, head_size
        ),
        lax.all_gather(values, "sp", axis=0, tiled=True).reshape(
            row_count // block_rows, block_rows, head_count, value_size
        ),
    )

    def advance(current, block_keys):
        return (
            (
                map_update(current[0], queries_first, block_keys[0], block_keys[2], score_scale),
                map_update(current[1], queries_second, block_keys[1], block_keys[2], score_scale),
            ),
            None,
        )

    statistics = lax.scan(advance, start_state, blocks)[0]

    def finish(map_stats):
        return map_stats[2] / map_stats[1].T[:, :, None]

    difference = finish(statistics[0]) - lambda_weight[None, :, None] * finish(statistics[1])
    scaled = difference * lax.rsqrt(
        jnp.mean(difference * difference, axis=-1, keepdims=True) + epsilon
    )
    attended = (
        (scaled * head_gain).astype(jnp.bfloat16).reshape(tokens_here, head_count * value_size)
    )
    partial_value = lax.dot_general(
        attended,
        lax.all_gather(out_weight, "sp", axis=0, tiled=True),
        (((1,), (1,)), ((), ())),
        preferred_element_type=jnp.float32,
    )
    summed = lax.psum_scatter(
        partial_value.astype(jnp.bfloat16), "tp", scatter_dimension=0, tiled=True
    ).astype(jnp.float32)
    after_attention = (residual.astype(jnp.float32) + summed).astype(jnp.bfloat16)
    stream = after_attention.astype(jnp.float32)
    scaled_rows = stream * lax.rsqrt(jnp.mean(stream * stream, axis=-1, keepdims=True) + epsilon)
    shard_piece = lax.all_gather(
        (scaled_rows * norm_gain).astype(jnp.bfloat16), "tp", axis=0, tiled=True
    )
    gate_part = jnp.dot(shard_piece, gate_weight, preferred_element_type=jnp.float32)
    up_part = jnp.dot(shard_piece, up_weight, preferred_element_type=jnp.float32)
    hidden = (jax.nn.silu(gate_part) * up_part).astype(jnp.bfloat16)
    down_partial = lax.dot_general(
        hidden,
        lax.all_gather(down_weight, "sp", axis=0, tiled=True),
        (((1,), (1,)), ((), ())),
        preferred_element_type=jnp.float32,
    )
    feed_out = lax.psum_scatter(
        down_partial.astype(jnp.bfloat16), "tp", scatter_dimension=0, tiled=True
    ).astype(jnp.float32)
    return (after_attention.astype(jnp.float32) + feed_out).astype(jnp.bfloat16)


def deal_body(*refs, sp_size, tp_size):
    sources, out_ref, extra_ref, arrived, sems = refs[:7], refs[7], refs[8], refs[9:16], refs[16]
    copies = [
        pltpu.make_async_copy(source, to, sems.at[index])
        for index, (source, to) in enumerate(zip(sources, arrived))
    ]
    for copy in copies:
        copy.start()
    for copy in copies:
        copy.wait()
    qf_ref, kf_ref, qs_ref, ks_ref, v_ref, gain_ref, lambda_ref = arrived
    here = lax.axis_index("sp") // 2
    member = lax.axis_index("tp")
    heads = sp_size // 2
    rows = qf_ref.shape[0] // tp_size
    size = qf_ref.shape[1] // heads
    value_size = v_ref.shape[1] // heads
    extra_ref[0:1] = gain_ref[...]
    extra_ref[1:2] = jnp.full((1, value_size), lambda_ref[here], jnp.float32)
    for block in range(tp_size):
        at = pl.ds(pl.multiple_of((member ^ block) * rows, rows), rows)
        for head in range(heads):
            columns = slice(head * size, (head + 1) * size)
            narrow = [ref[at, columns] for ref in (qf_ref, qs_ref, kf_ref, ks_ref)]
            out_ref[here ^ head, block * rows : (block + 1) * rows, :] = jnp.concatenate(
                narrow + [v_ref[at, head * value_size : (head + 1) * value_size]], axis=1
            )


def attention_body(
    extra_ref, a_ref, b_ref, c_ref, d_ref, ab_ref, cd_ref, out_ref, k_ref, v_ref
):
    rows = a_ref.shape[0]
    gain, weight = extra_ref[0:1], extra_ref[1:2]
    lanes = a_ref.shape[1] - ab_ref.shape[1]
    head_size = lanes // 2
    scale = head_size ** (-0.5)
    exact = math.frexp(scale)[0] == 0.5
    queries = (a_ref, b_ref, c_ref, d_ref)
    for index, ref in enumerate(queries):
        k_ref[index * rows : (index + 1) * rows] = ref[:, lanes : 2 * lanes]
        v_ref[index * rows : (index + 1) * rows] = ref[:, 2 * lanes :]
    start = len(queries) * rows
    for ref in (ab_ref, cd_ref):
        at = slice(start, start + ref.shape[0])
        start += ref.shape[0]
        k_ref[at] = ref[:, :lanes]
        v_ref[at] = ref[:, lanes:]
    lane = lax.broadcasted_iota(jnp.int32, (rows, lanes), 1)

    def one_map(query, which):
        wanted = (lane < head_size) if which == 0 else (lane >= head_size)
        scores = lax.dot_general(
            jnp.where(wanted, query, jnp.zeros_like(query)),
            k_ref[...],
            (((1,), (1,)), ((), ())),
            preferred_element_type=jnp.float32,
        )
        if not exact:
            scores = scores * scale
        shifted = jnp.exp(scores - scores.max(axis=-1, keepdims=True))
        total = shifted.sum(axis=-1, keepdims=True)
        product = jnp.dot(
            shifted.astype(jnp.bfloat16), v_ref[...], preferred_element_type=jnp.float32
        )
        return product / total

    for index, ref in enumerate(queries):
        query = ref[:, :lanes]
        if exact:
            query = query * jnp.asarray(scale, query.dtype)
        difference = one_map(query, 0) - weight * one_map(query, 1)
        scaled = difference * lax.rsqrt(
            jnp.mean(difference * difference, axis=-1, keepdims=True) + epsilon
        )
        out_ref[index] = (scaled * gain).astype(out_ref.dtype)


def project_body(
    a_ref, b_ref, c_ref, d_ref, other_ref, source, kept_ref, sent_ref, own_ref, heads_ref, sem, *, tp_size
):
    copy = pltpu.make_async_copy(source, own_ref, sem)
    copy.start()
    here = lax.axis_index("sp") // 2
    planes, tokens, size = a_ref.shape
    for distance, ref in enumerate((a_ref, b_ref, c_ref, d_ref)):
        columns = pl.ds(pl.multiple_of((here ^ distance) * size, size), size)
        for block in range(planes):
            heads_ref[block * tokens : (block + 1) * tokens, columns] = ref[distance ^ block]
    rows = tokens // tp_size
    width = own_ref.shape[0]
    for index, ref in ((1, other_ref), (0, own_ref)):
        if index == 0:
            copy.wait()
        columns = slice(index * width, (index + 1) * width)
        product = lax.dot_general(
            heads_ref[...], ref[...], (((1,), (1,)), ((), ())), preferred_element_type=jnp.float32
        )
        for block in range(planes):
            for chip in range(tp_size // 2):
                to = slice((chip * planes + block) * rows, (chip * planes + block + 1) * rows)
                at = block * tokens + chip * 2 * rows
                kept_ref[to, columns] = product[at : at + rows]
                sent_ref[to, columns] = product[at + rows : at + 2 * rows].astype(sent_ref.dtype)


def gate_body(here_ref, there_ref, gate_ref, up_ref, hidden_ref, both_ref, *rest, tile):
    rows = here_ref.shape[0]
    units = gate_ref.shape[1]
    starts = range(0, units, tile)
    buffers, sems = rest[:-1], rest[-1]
    copies = []
    for index, start in enumerate(starts):
        columns = pl.ds(start, min(tile, units - start))
        pair = [
            pltpu.make_async_copy(
                ref.at[:, columns], buffers[2 * index + which], sems.at[2 * index + which]
            )
            for which, ref in enumerate((gate_ref, up_ref))
        ]
        for copy in pair:
            copy.start()
        copies.append(pair)
    both_ref[:rows] = here_ref[...]
    both_ref[rows:] = there_ref[...]
    for index, start in enumerate(starts):
        for copy in copies[index]:
            copy.wait()
        gate, up = (
            jnp.dot(
                both_ref[...], buffers[2 * index + which][...], preferred_element_type=jnp.float32
            )
            for which in range(2)
        )
        hidden = gate / (1.0 + jnp.exp(-gate)) * up
        hidden_ref[:, start : start + gate.shape[1]] = hidden.astype(hidden_ref.dtype)


def down_body(hidden_ref, *refs, pieces, sp_size):
    kept_ref, sent_ref = refs[-2:]
    refs = list(refs[:-2])
    place = lax.axis_index("sp") // 2
    inner = (place > 0) & (place < sp_size // 2 - 1)
    rows = kept_ref.shape[0]
    start = 0
    for parts, choices in pieces:
        values = []
        for _ in range(parts):
            part = [refs.pop(0)[...] for _ in range(choices)]
            values.append(part[0] if choices == 1 else jnp.where(inner, *part))
        piece = values[0] if parts == 1 else jnp.concatenate(values, axis=0)
        product = lax.dot_general(
            hidden_ref[...], piece, (((1,), (1,)), ((), ())), preferred_element_type=jnp.float32
        )
        columns = slice(start, start + piece.shape[0])
        kept_ref[:, columns] = product[:rows]
        sent_ref[:, columns] = product[rows:].astype(sent_ref.dtype)
        start += piece.shape[0]


def kernel(body, out_shape, near, away=(), scratch=(), limit=16):
    vmem = pl.BlockSpec(memory_space=pltpu.VMEM)
    many = isinstance(out_shape, tuple)
    call = pl.pallas_call(
        body,
        out_shape=out_shape,
        in_specs=[vmem] * len(near) + [pl.BlockSpec(memory_space=pltpu.HBM)] * len(away),
        out_specs=(vmem,) * len(out_shape) if many else vmem,
        scratch_shapes=list(scratch),
        compiler_params=pltpu.CompilerParams(vmem_limit_bytes=limit * 2**20),
    )
    return call(*near, *(pltpu.with_memory_space_constraint(array, pltpu.HBM) for array in away))


def moved_local(
    sp_size,
    tp_size,
    residual,
    query_first,
    key_first,
    query_second,
    key_second,
    values,
    lambda_weight,
    head_gain,
    out_weight,
    norm_gain,
    gate_weight,
    up_weight,
    down_weight,
):
    side, near, across, far = 1, 2, sp_size // 2, sp_size - 2
    planes = sp_size // 2
    chip, core = tp_size // 2, 1
    place = lax.axis_index("sp")
    on_side = (place & 1) == 1
    low = (place & 2) == 2
    high = (place & 4) == 4
    bf16, f32 = jnp.bfloat16, jnp.float32

    def swap(array, axis, distance):
        count = sp_size if axis == "sp" else tp_size
        return lax.ppermute(array, axis, [(i, i ^ distance) for i in range(count)])

    def swap_both(array, first, second):
        pairs = [
            (i * tp_size + j, (i ^ first) * tp_size + (j ^ second))
            for i in range(sp_size)
            for j in range(tp_size)
        ]
        return lax.ppermute(array, ("sp", "tp"), pairs)

    inner = [i for i in range(sp_size) if 0 < i // 2 < planes - 1]
    middle_pairs = [(i, i ^ far) for i in inner]
    outward_pairs = [(i, i ^ near) for i in inner]

    def three(first, second, third):
        third = swap(third, "sp", far)
        second = swap(second, "sp", across)
        return swap(first, "sp", near), second, third

    def along_line(weight):
        near_one = swap(weight, "sp", near)
        middle_one = lax.ppermute(weight, "sp", middle_pairs)
        middle_two = lax.ppermute(near_one, "sp", middle_pairs)
        outer_one = lax.ppermute(middle_one, "sp", outward_pairs)
        outer_two = lax.ppermute(middle_two, "sp", outward_pairs)
        return near_one, middle_one, outer_one, middle_two, outer_two

    def planes_by_distance(n):
        n = [jnp.where(low, n[k ^ 1], n[k]) for k in range(4)]
        return [jnp.where(high, n[k ^ 2], n[k]) for k in range(4)]

    def planes_along_line(n):
        first, second = jnp.where(low, n[1], n[0]), jnp.where(low, n[0], n[1])
        return [
            jnp.where(high, n[3], first),
            jnp.where(high, n[2], second),
            jnp.where(high, first, n[2]),
            jnp.where(high, second, n[3]),
        ]

    def side_by_side(same, other):
        return jnp.concatenate(
            [jnp.where(on_side, other, same), jnp.where(on_side, same, other)], axis=1
        )

    def plane_sum(ours, given_away):
        ours = ours + swap(given_away, "tp", core).astype(f32)
        half_rows = ours.shape[0] // 2
        from_chip = swap(ours[half_rows:].astype(bf16), "tp", chip)
        ours = ours[:half_rows] + from_chip.astype(f32)
        rows = half_rows // planes
        blocks = [ours[k * rows : (k + 1) * rows] for k in range(planes)]
        others = three(*(block.astype(bf16) for block in blocks[1:]))
        blocks = [blocks[0], *(block.astype(f32) for block in others)]
        middle = ours.shape[1] // 2
        blocks = [side_by_side(block[:, :middle], block[:, middle:]) for block in blocks]
        return jnp.concatenate(planes_by_distance(blocks), axis=1)

    def side_parts(ours, given_away):
        ours = ours + swap(given_away, "tp", core).astype(f32)
        rows = ours.shape[0] // 4
        rounded = ours.astype(bf16)
        from_both = swap_both(rounded[3 * rows :], side, chip)
        from_side = swap(rounded[2 * rows : 3 * rows], "sp", side)
        from_chip = swap(rounded[rows : 2 * rows], "tp", chip)
        return ours[:rows], from_chip, from_side, from_both

    def side_sum(own, from_chip, from_side, from_both):
        return own + from_chip.astype(f32), from_side.astype(f32) + from_both.astype(f32)

    tokens = query_first.shape[0]
    rows = tokens // tp_size
    head_lanes = 2 * query_first.shape[1] // planes
    value_size = head_gain.shape[0]

    streams = (query_first, key_first, query_second, key_second, values)
    dealt, extra = kernel(
        functools.partial(deal_body, sp_size=sp_size, tp_size=tp_size),
        (
            jax.ShapeDtypeStruct((planes, tokens, 2 * head_lanes + value_size), bf16),
            jax.ShapeDtypeStruct((2, value_size), f32),
        ),
        (),
        (*streams, head_gain.reshape(1, -1), lambda_weight),
        [pltpu.VMEM(array.shape, bf16) for array in streams]
        + [
            pltpu.VMEM((1, value_size), f32),
            pltpu.SMEM(lambda_weight.shape, f32),
            pltpu.SemaphoreType.DMA((7,)),
        ],
    )
    first, second, third = three(dealt[1], dealt[2], dealt[3])
    early = swap(dealt[0][:, head_lanes:], "sp", side)
    late = swap(
        jnp.concatenate([block[:, head_lanes:] for block in (first, second, third)], 0), "sp", side
    )
    attended = kernel(
        attention_body,
        jax.ShapeDtypeStruct((planes, tokens, value_size), bf16),
        (extra, dealt[0], first, second, third, early, late),
        scratch=[
            pltpu.VMEM((2 * planes * tokens, head_lanes), bf16),
            pltpu.VMEM((2 * planes * tokens, value_size), bf16),
        ],
    )
    width = residual.shape[1]
    part = (planes * tokens // 2, width // planes)
    projected = kernel(
        functools.partial(project_body, tp_size=tp_size),
        (jax.ShapeDtypeStruct(part, f32), jax.ShapeDtypeStruct(part, bf16)),
        (attended, *three(attended, attended, attended), swap(out_weight, "sp", side)),
        (out_weight,),
        [
            pltpu.VMEM(out_weight.shape, bf16),
            pltpu.VMEM((planes * tokens, out_weight.shape[1]), bf16),
            pltpu.SemaphoreType.DMA,
        ],
    )
    summed = plane_sum(*projected)
    after_attention = (residual.astype(f32) + summed).astype(bf16)
    stream = after_attention.astype(f32)
    scaled_rows = stream * lax.rsqrt(jnp.mean(stream * stream, axis=-1, keepdims=True) + epsilon)
    normed = (scaled_rows * norm_gain).astype(bf16)

    from_both = swap_both(normed, side, chip)
    from_side = swap(normed, "sp", side)
    from_chip = swap(normed, "tp", chip)
    four = jnp.concatenate([normed, from_chip, from_side, from_both], axis=0)
    units = gate_weight.shape[1]
    tile = 256
    sizes = [min(tile, units - start) for start in range(0, units, tile) for _ in range(2)]
    hidden = kernel(
        functools.partial(gate_body, tile=tile),
        jax.ShapeDtypeStruct((8 * rows, units), bf16),
        (four, swap(four, "tp", core)),
        (gate_weight, up_weight),
        [pltpu.VMEM((8 * rows, residual.shape[1]), bf16)]
        + [pltpu.VMEM((residual.shape[1], size), bf16) for size in sizes]
        + [pltpu.SemaphoreType.DMA((len(sizes),))],
        limit=24,
    )
    middle = down_weight.shape[0] * 5 // 8
    ways = [along_line(down_weight[:middle]), along_line(down_weight[middle:])]

    def project_down(pieces, operands, columns):
        shape = (4 * rows, columns)
        parts = kernel(
            functools.partial(down_body, pieces=pieces, sp_size=sp_size),
            (jax.ShapeDtypeStruct(shape, f32), jax.ShapeDtypeStruct(shape, bf16)),
            (hidden, *operands),
        )
        return side_parts(*parts)

    piece = down_weight.shape[0]
    early_refs = [down_weight, *(way[0] for way in ways)]
    early_refs += [ref for way in ways for ref in way[1:3]]
    first = project_down(((1, 1), (2, 1), (2, 2)), early_refs, 3 * piece)
    last = project_down(((2, 2),), [ref for way in ways for ref in way[3:5]], piece)
    first, last = lax.optimization_barrier((first, last))
    first, last = side_sum(*first), side_sum(*last)
    joined = [
        side_by_side(*(array[:, k * piece : (k + 1) * piece] for array in first)) for k in range(3)
    ]
    joined.append(side_by_side(*last))
    fed = jnp.concatenate(planes_along_line(joined), axis=1)
    return (stream + fed).astype(bf16)


def solution(mesh):
    sp_size, tp_size = mesh.shape["sp"], mesh.shape["tp"]

    def local(*arrays):
        total_tokens = arrays[1].shape[0] * sp_size
        short = total_tokens <= arrays[0].shape[1]
        if short and (sp_size, tp_size) == (8, 4):
            return moved_local(sp_size, tp_size, *arrays)
        return gathered_local(*arrays)

    return jax.shard_map(
        local,
        mesh=mesh,
        in_specs=(
            P(("sp", "tp"), None),
            P("sp", "tp"),
            P("sp", "tp"),
            P("sp", "tp"),
            P("sp", "tp"),
            P("sp", "tp"),
            P("tp"),
            P(),
            P("sp", "tp"),
            P(),
            P(None, "tp"),
            P(None, "tp"),
            P("sp", "tp"),
        ),
        out_specs=P(("sp", "tp"), None),
        check_vma=False,
    )
```
